128 devices in a mesh: ep: 128 (over z, y, x, core).
Axes of the slice: x: 4, y: 4, z: 4, core: 2. Of those that a mesh axis runs over, the one named last changes fastest.
Arguments:
- tokens: bfloat16 [6144, 2048], P('ep'), may hold values from -6 to 6
- history_length: int32 [6144], P('ep'), may hold values from 1024 to 8192
- norm_gain: float32 [2048], replicated, may hold values from 0.1 to 1.9
- w_query: bfloat16 [2048, 512], replicated, may hold values from -0.125 to 0.125
- w_key: bfloat16 [2048, 512], replicated, may hold values from -0.125 to 0.125
- w_value: bfloat16 [2048, 512], replicated, may hold values from -0.125 to 0.125
- w_gate: bfloat16 [2048, 512], replicated, may hold values from -0.125 to 0.125
- decay_rate: float32 [8], replicated, may hold values from 0.003 to 0.7
- state: float32 [6144, 8, 64, 64], P('ep'), may hold values from -4 to 4
- head_gain: float32 [512], replicated, may hold values from 0.1 to 1.9
- w_out: bfloat16 [512, 2048], replicated, may hold values from -0.25 to 0.25
- moe_gain: float32 [2048], replicated, may hold values from 0.1 to 1.9
- route_weights: float32 [6144, 2], P('ep'), may hold values from 0.3 to 3
- expert_group: int32 [6144], P('ep'), may hold values from 0 to 3, as said below
- expert_inner: int32 [6144, 2], P('ep'), may hold values from 0 to 31, as said below
- expert_gate: bfloat16 [128, 2048, 256], P('ep'), may hold values from -0.125 to 0.125
- expert_up: bfloat16 [128, 2048, 256], P('ep'), may hold values from -0.125 to 0.125
- expert_down: bfloat16 [128, 256, 2048], P('ep'), may hold values from -0.375 to 0.375
Outputs:
- output: bfloat16 [6144, 2048], P('ep')
- new_state: float32 [6144, 8, 64, 64], P('ep')
The draws below stay inside these ranges and needn't reach their ends.
Inputs may be any that keep to these rules, and one draw needn't show every extreme that they name: `expert_group`: together with expert_inner it names 2 different experts of one group for each token. `expert_inner`: the rows of one device name one expert at most 2 times; in every draw some expert is named exactly 2 times by the rows of every device.
All inputs are finite; a program needn't handle non-finite values.
Results may differ from the reference program's by a relative error of at most 0.02.
Values may be sent and summed in bfloat16 or wider, within the bound.
No kernel may reach another device: no remote copies, remote signals or barrier semaphores. Data moves between devices by JAX's collectives and lax.ppermute only.
A program may use at most 128 MiB of HBM per device.

```python
import math
import jax
import jax.numpy as jnp
from jax import lax

D = 2048
HEADS = 8
HEAD_DIM = 64
RET_WIDTH = 512
EXPERT_WIDTH = 256
SEQ_DEV = 48
TOKENS = 6144
EXPERTS = 128
GROUPS = 4
GROUP_SIZE = 32
TOP_K = 2
CAP = 2
N_EP = 128


def route_table(key):
    root_key = jax.random.fold_in(key, 7)
    pair_count = EXPERTS * CAP // 2
    per_group = pair_count // GROUPS
    hot_group = jax.random.randint(jax.random.fold_in(root_key, 1), (), 0, GROUPS)
    relabel = jax.vmap(lambda subkey: jax.random.permutation(subkey, GROUP_SIZE))(jax.random.split(jax.random.fold_in(root_key, 2), GROUPS))
    pair_ids = jnp.arange(pair_count, dtype=jnp.int32)
    pair_group = pair_ids // per_group
    pair_offset = pair_ids % per_group
    first_inner = relabel[pair_group, 2 * pair_offset % GROUP_SIZE]
    second_inner = relabel[pair_group, (2 * pair_offset + 1) % GROUP_SIZE]
    heated = (pair_group == hot_group) & (pair_offset % (GROUP_SIZE // 2) == 0)

    def one_block(subkey):
        jitter = jax.random.randint(jax.random.fold_in(subkey, 1), (pair_count,), 0, 1 << 20)
        scores = jnp.where(heated, pair_ids, (jitter + 1) * pair_count + pair_ids)
        _, chosen = lax.top_k(-scores, SEQ_DEV)
        chosen = chosen[jax.random.permutation(jax.random.fold_in(subkey, 2), SEQ_DEV)]
        return (pair_group[chosen], jnp.stack([first_inner[chosen], second_inner[chosen]], axis=-1))
    groups, inner_ids = jax.vmap(one_block)(jax.random.split(jax.random.fold_in(root_key, 3), TOKENS // SEQ_DEV))
    return (groups.reshape(TOKENS).astype(jnp.int32), inner_ids.reshape(TOKENS, TOP_K).astype(jnp.int32))


def draw_expert_group(key, part):
    return route_table(key)[0]


def draw_expert_inner(key, part):
    return route_table(key)[1]


def place_ends(result, own_key, least, largest):
    dims = result.shape
    index_at = [jax.random.randint(jax.random.fold_in(own_key, axis), (), 0, dims[axis]) for axis in range(len(dims))]
    result = result.at[tuple(index_at)].set(least)
    longest = dims.index(max(dims))
    index_at[longest] = (index_at[longest] + 1) % dims[longest]
    return result.at[tuple(index_at)].set(largest)


def block_levels(own_key, extent, cuts, low, high):
    level = 1.0
    for position, shards_of in cuts:
        steps = jax.random.uniform(jax.random.fold_in(jax.random.fold_in(own_key, 6), position), (shards_of,), jnp.float32, low / len(cuts), high / len(cuts))
        level = level * jnp.repeat(jnp.exp(steps), extent[position] // shards_of).reshape((-1,) + (1,) * (len(extent) - 1 - position))
    return level


def normal_values(own_key, extent, scale, most, cuts=(), held_as=jnp.bfloat16):
    values = scale * jax.random.normal(own_key, extent, jnp.float32)
    if cuts:
        values = values * block_levels(own_key, extent, cuts, -0.22, 0.18)
    return jnp.clip(values, -most, most).astype(held_as)


def setup_inputs(seed: int = 0) -> dict:
    key_list = jax.random.split(jax.random.key(seed), 19)
    return {
        "tokens": normal_values(key_list[0], (TOKENS, D), 1.0, 6.0, ((0, 128),)),
        "history_length": place_ends(jax.random.randint(key_list[1], (TOKENS,), 1024, 8193), jax.random.fold_in(key_list[1], 1), 1024, 8192).astype(jnp.int32),
        "norm_gain": jnp.clip(1.0 + 0.18 * jax.random.normal(key_list[2], (D,), jnp.float32), 0.1, 1.9),
        "w_query": normal_values(key_list[3], (D, RET_WIDTH), D ** -0.5, 0.125),
        "w_key": normal_values(key_list[4], (D, RET_WIDTH), D ** -0.5, 0.125),
        "w_value": normal_values(key_list[5], (D, RET_WIDTH), D ** -0.5, 0.125),
        "w_gate": normal_values(key_list[6], (D, RET_WIDTH), D ** -0.5, 0.125),
        "decay_rate": jnp.clip(jnp.exp(jax.random.uniform(key_list[7], (HEADS,), jnp.float32, math.log(0.003), math.log(0.7))), 0.003, 0.7),
        "state": normal_values(key_list[8], (TOKENS, HEADS, HEAD_DIM, HEAD_DIM), 0.3, 4.0, ((0, 128),), jnp.float32),
        "head_gain": jnp.clip(1.0 + 0.18 * jax.random.normal(key_list[9], (RET_WIDTH,), jnp.float32), 0.1, 1.9),
        "w_out": normal_values(key_list[10], (RET_WIDTH, D), RET_WIDTH ** -0.5, 0.25),
        "moe_gain": jnp.clip(1.0 + 0.18 * jax.random.normal(key_list[11], (D,), jnp.float32), 0.1, 1.9),
        "route_weights": jnp.clip(jnp.exp(math.log(3.0) - 2.3025851 * jax.random.uniform(key_list[12], (TOKENS, TOP_K), jnp.float32) ** block_levels(key_list[12], (TOKENS, TOP_K), ((0, 128),), -0.2, 0.2)), 0.3, 3.0),
        "expert_group": draw_expert_group(jax.random.fold_in(key_list[18], 71), 0),
        "expert_inner": draw_expert_inner(jax.random.fold_in(key_list[18], 71), 0),
        "expert_gate": normal_values(key_list[15], (EXPERTS, D, EXPERT_WIDTH), D ** -0.5, 0.125, ((0, 128),)),
        "expert_up": normal_values(key_list[16], (EXPERTS, D, EXPERT_WIDTH), D ** -0.5, 0.125, ((0, 128),)),
        "expert_down": normal_values(key_list[17], (EXPERTS, EXPERT_WIDTH, D), EXPERT_WIDTH ** -0.5, 0.375, ((0, 128),)),
    }


epsilon = 1e-06

def rotate(values, places):
    halfway = values.shape[-1] // 2
    inverse = 10000.0 ** (-jnp.arange(halfway, dtype=jnp.float32) / halfway)
    angles = places[:, None] * inverse[None, :]
    cosine = jnp.cos(angles)[:, None, :]
    sine_table = jnp.sin(angles)[:, None, :]
    first_half = values[..., :halfway]
    second = values[..., halfway:]
    return jnp.concatenate([first_half * cosine - second * sine_table, first_half * sine_table + second * cosine], axis=-1)

def rms_scale(values, gains):
    return values * lax.rsqrt(lax.optimization_barrier(jnp.mean(values * values, axis=-1, keepdims=True)) + epsilon) * gains

def retention_step(tokens, history_length, norm_gain, w_query, w_key, w_value, w_gate, decay_rate, state, head_gain, w_out, moe_gain):
    row_count = tokens.shape[0]
    head_count = decay_rate.shape[0]
    head_width = state.shape[-1]
    inputs = tokens.astype(jnp.float32)
    normed = rms_scale(inputs, norm_gain).astype(jnp.bfloat16)

    def project(weights):
        return jnp.dot(normed, weights, preferred_element_type=jnp.float32).astype(jnp.bfloat16)
    queries = project(w_query).reshape(row_count, head_count, head_width).astype(jnp.float32)
    keys_now = project(w_key).reshape(row_count, head_count, head_width).astype(jnp.float32)
    values_now = project(w_value).reshape(row_count, head_count, head_width).astype(jnp.float32)
    gating = project(w_gate).astype(jnp.float32)
    places = history_length.astype(jnp.float32)
    queries = rotate(queries, places)
    keys_now = rotate(keys_now, places) * head_width ** (-0.5)
    retain = jnp.exp(-decay_rate)
    new_state = retain[None, :, None, None] * state + keys_now[:, :, :, None] * values_now[:, :, None, :]
    reading = jnp.einsum('bhk,bhkv->bhv', queries, new_state, precision=lax.Precision.HIGHEST)
    reading = rms_scale(reading, head_gain.reshape(head_count, head_width))
    mixed_heads = (reading.reshape(row_count, head_count * head_width) * jax.nn.silu(gating)).astype(jnp.bfloat16)
    mixed_tokens = (inputs + jnp.dot(mixed_heads, w_out, preferred_element_type=jnp.float32)).astype(jnp.bfloat16)
    normed_moe = rms_scale(mixed_tokens.astype(jnp.float32), moe_gain).astype(jnp.bfloat16)
    return (mixed_tokens, normed_moe, new_state)

def expert_apply(row_block, gate_weight, up_weight, down_weight):
    gate_part = jnp.dot(row_block, gate_weight, preferred_element_type=jnp.float32)
    up_part = jnp.dot(row_block, up_weight, preferred_element_type=jnp.float32)
    hidden = (jax.nn.silu(gate_part) * up_part).astype(jnp.bfloat16)
    return jnp.dot(hidden, down_weight, preferred_element_type=jnp.float32).astype(jnp.bfloat16)

def reference(tokens, history_length, norm_gain, w_query, w_key, w_value, w_gate, decay_rate, state, head_gain, w_out, moe_gain, route_weights, expert_group, expert_inner, expert_gate, expert_up, expert_down):
    mixed_tokens, normed_moe, new_state = retention_step(tokens, history_length, norm_gain, w_query, w_key, w_value, w_gate, decay_rate, state, head_gain, w_out, moe_gain)
    row_count = tokens.shape[0]
    experts = expert_gate.shape[0]
    per_group = experts // GROUPS
    flat_ids = (expert_group[:, None] * per_group + expert_inner).reshape(-1).astype(jnp.int32)
    slot_total = flat_ids.shape[0]
    padded_ids = jnp.concatenate([flat_ids, jnp.full((1,), -1, jnp.int32)])
    owners = jnp.concatenate([jnp.arange(slot_total, dtype=jnp.int32) // TOP_K, jnp.zeros((1,), jnp.int32)])
    scales = jnp.concatenate([route_weights.reshape(-1), jnp.zeros((1,), jnp.float32)])
    row_bound = N_EP * CAP

    def visit_expert(running, expert):
        matched = padded_ids == expert
        picked = jnp.nonzero(matched, size=row_bound, fill_value=slot_total)[0].astype(jnp.int32)
        owner_rows = owners[picked]
        weighting = jnp.where(matched[picked], scales[picked], jnp.zeros_like(scales[picked]))
        outputs = expert_apply(normed_moe[owner_rows], expert_gate[expert], expert_up[expert], expert_down[expert])
        running = running.at[owner_rows].add(outputs.astype(jnp.float32) * weighting[:, None])
        return (running, None)
    running, _ = lax.scan(visit_expert, jnp.zeros((row_count, tokens.shape[1]), jnp.float32), jnp.arange(experts, dtype=jnp.int32))
    output = (mixed_tokens.astype(jnp.float32) + running).astype(jnp.bfloat16)
    return (output, new_state)
```

```python
import functools

import jax
import jax.numpy as jnp
import numpy as np
from jax import lax
from jax.experimental import pallas as pl
from jax.experimental.pallas import tpu as pltpu
from jax.sharding import PartitionSpec as P

EPS = 1e-06
ROWS = 48
D = 2048
HEADS = 8
HD = 64
RW = HEADS * HD
EXPERTS = 128
PER_GROUP = 32
LANES = 128
TILES = D // LANES
GROUP = 8
CHUNKS = ROWS // GROUP
F32 = jnp.float32
BF16 = jnp.bfloat16


def lane_iota(shape):
    return lax.broadcasted_iota(jnp.int32, shape, len(shape) - 1)


def group_sum(x, ones):
    high = x.astype(BF16)
    low = (x - high.astype(F32)).astype(BF16)
    return jnp.dot(high, ones, preferred_element_type=F32) + jnp.dot(
        low, ones, preferred_element_type=F32
    )


def rope(x, cosine, sine):
    lanes = lane_iota((ROWS, LANES))
    first = (lanes % HD) < (HD // 2)
    parts = []
    for c in range(RW // LANES):
        part = x[:, c * LANES : (c + 1) * LANES]
        other = jnp.where(
            first,
            pltpu.roll(part, LANES - HD // 2, 1),
            pltpu.roll(part, HD // 2, 1),
        )
        parts.append(part * cosine + other * jnp.where(first, -sine, sine))
    return jnp.concatenate(parts, axis=1)


def front_kernel(
    hist_hbm,
    inv_hbm,
    ngain_hbm,
    decay_hbm,
    hgain_hbm,
    mgain_hbm,
    group_hbm,
    inner_hbm,
    tok_hbm,
    wq_hbm,
    wk_hbm,
    wv_hbm,
    wg_hbm,
    state_hbm,
    wo_hbm,
    mixed_ref,
    send0_ref,
    send1_ref,
    k_ref,
    v_ref,
    hist,
    inv,
    ngain,
    decay,
    hgain,
    mgain,
    group,
    inner,
    tok,
    w4,
    wo,
    st,
    qs,
    part,
    wide,
    tiles,
    small_sem,
    w_sem,
    st_sem,
):
    small = [
        pltpu.make_async_copy(tok_hbm, tok, small_sem.at[0]),
        pltpu.make_async_copy(ngain_hbm, ngain, small_sem.at[1]),
        pltpu.make_async_copy(hist_hbm, hist, small_sem.at[2]),
        pltpu.make_async_copy(inv_hbm, inv, small_sem.at[3]),
        pltpu.make_async_copy(decay_hbm, decay, small_sem.at[4]),
        pltpu.make_async_copy(hgain_hbm, hgain, small_sem.at[5]),
        pltpu.make_async_copy(mgain_hbm, mgain, small_sem.at[6]),
        pltpu.make_async_copy(group_hbm, group, small_sem.at[7]),
        pltpu.make_async_copy(inner_hbm, inner, small_sem.at[8]),
    ]
    for copy in small:
        copy.start()
    weights = [
        pltpu.make_async_copy(src, w4.at[i], w_sem.at[i])
        for i, src in enumerate((wq_hbm, wk_hbm, wv_hbm, wg_hbm))
    ]
    for copy in weights:
        copy.start()
    states = [
        pltpu.make_async_copy(
            state_hbm.at[pl.ds(i * GROUP, GROUP)],
            st.at[pl.ds(i * GROUP, GROUP)],
            st_sem.at[i],
        )
        for i in range(CHUNKS)
    ]
    for copy in states:
        copy.start()
    wo_copy = pltpu.make_async_copy(wo_hbm, wo, w_sem.at[4])
    wo_copy.start()
    for copy in small:
        copy.wait()

    x = tok[...].astype(F32)
    scale = lax.rsqrt(jnp.mean(x * x, axis=-1, keepdims=True) + EPS)
    normed = (x * scale * ngain[...]).astype(BF16)

    square = (ROWS, ROWS)
    place = jnp.sum(
        jnp.where(
            lax.broadcasted_iota(jnp.int32, square, 0) == lane_iota(square),
            jnp.broadcast_to(hist[...].astype(F32), square),
            0.0,
        ),
        axis=1,
        keepdims=True,
    )
    angles = place * inv[...]
    cosine = jnp.cos(angles)
    sine = jnp.sin(angles)

    zero = jnp.zeros((TILES, LANES), BF16)
    for e in range(EXPERTS):
        send0_ref[e] = zero
        send1_ref[e] = zero

    def project(i):
        weights[i].wait()
        return jnp.dot(normed, w4[i], preferred_element_type=F32).astype(BF16).astype(F32)

    q = rope(project(0), cosine, sine)
    qs[...] = q
    k = rope(project(1), cosine, sine) * (HD**-0.5)
    k_ref[...] = k
    v = project(2)
    v_ref[...] = v
    gate = project(3)

    ones = (
        lax.broadcasted_iota(jnp.int32, (RW, RW), 0) // HD == lane_iota((RW, RW)) // HD
    ).astype(BF16)
    fresh = group_sum(q * k, ones) * v
    heads = lane_iota((1, RW)) // HD
    rate = jnp.zeros((1, RW), F32)
    for h in range(HEADS):
        rate = jnp.where(heads == h, decay[h], rate)
    retain = jnp.exp(-rate)

    def chunk(i, carry):
        pltpu.make_async_copy(
            state_hbm.at[pl.ds(i * GROUP, GROUP)],
            st.at[pl.ds(i * GROUP, GROUP)],
            st_sem.at[i],
        ).wait()
        start = pl.multiple_of(i * GROUP, GROUP)
        qt = qs[pl.ds(start, GROUP), :].T
        for b in range(GROUP):
            for h in range(HEADS):
                column = qt[h * HD : (h + 1) * HD, b : b + 1]
                product = st[i * GROUP + b, h] * column
                total = product[0:8]
                for r in range(1, 8):
                    total = total + product[r * 8 : r * 8 + 8]
                part[
                    pl.ds(pl.multiple_of((h * ROWS + i * GROUP + b) * 8, 8), 8), 0:HD
                ] = total
        return carry

    lax.fori_loop(0, CHUNKS, chunk, 0)

    def head_rows(h):
        total = part[pl.ds(h * ROWS * 8, ROWS, stride=8), :]
        for s in range(1, 8):
            total = total + part[pl.ds(h * ROWS * 8 + s, ROWS, stride=8), :]
        return total

    low_half = lane_iota((ROWS, LANES)) < HD
    old = jnp.concatenate(
        [
            jnp.where(
                low_half, head_rows(2 * c), pltpu.roll(head_rows(2 * c + 1), HD, 1)
            )
            for c in range(HEADS // 2)
        ],
        axis=1,
    )
    reading = retain * old + fresh
    mean_square = group_sum(reading * reading, ones) * (1.0 / HD)
    reading = reading * lax.rsqrt(mean_square + EPS) * hgain[...]
    mixed_heads = (reading * jax.nn.silu(gate)).astype(BF16)
    wo_copy.wait()
    mixed = (x + jnp.dot(mixed_heads, wo[...], preferred_element_type=F32)).astype(BF16)
    mixed = mixed.astype(F32)
    scale = lax.rsqrt(jnp.mean(mixed * mixed, axis=-1, keepdims=True) + EPS)
    normed_moe = mixed * scale * mgain[...]

    for r in range(TILES):
        wide[pl.ds(r, ROWS, stride=TILES), :] = normed_moe[:, r * LANES : (r + 1) * LANES]
    tiles[...] = wide[...].astype(BF16).reshape(ROWS, TILES, LANES)
    for r in range(TILES):
        wide[pl.ds(r, ROWS, stride=TILES), :] = mixed[:, r * LANES : (r + 1) * LANES]
    mixed_ref[...] = wide[...].astype(BF16).reshape(ROWS, TILES, LANES)

    for t in range(ROWS):
        base = group[t] * PER_GROUP
        row = tiles[t]
        for j in range(2):
            send1_ref[base + inner[j, t]] = row
    for t in reversed(range(ROWS)):
        base = group[t] * PER_GROUP
        row = tiles[t]
        for j in (1, 0):
            send0_ref[base + inner[j, t]] = row


def state_kernel(
    decay, group, inner, weight, state_ref, k_ref, v_ref, new_ref, use_ref, seen
):
    kt = k_ref[...].T
    v = v_ref[...]
    for h in range(HEADS):
        retain = jnp.exp(jnp.full((HD, HD), -decay[h], F32))
        for b in range(GROUP):
            column = kt[h * HD : (h + 1) * HD, b : b + 1]
            row = v[b : b + 1, h * HD : (h + 1) * HD]
            new_ref[b, h] = retain * state_ref[b, h] + column * row

    @pl.when(pl.program_id(0) == 0)
    def _():
        def clear(e, carry):
            seen[e] = 0
            return carry

        lax.fori_loop(0, EXPERTS, clear, 0)

        def visit(t, carry):
            for j in range(2):
                e = group[t] * PER_GROUP + inner[j, t]
                slot = seen[e]
                seen[e] = 1
                w = weight[j, t]
                use_ref[0, j, t] = jnp.where(slot == 0, w, 0.0)
                use_ref[1, j, t] = jnp.where(slot == 0, 0.0, w)
            return carry

        lax.fori_loop(0, ROWS, visit, 0)


def expert_kernel(in_ref, wg_ref, wu_ref, wd_ref, out_ref, wide, lhs):
    n = in_ref.shape[0]
    wide[...] = in_ref[...].astype(F32).reshape(n * TILES, LANES)
    for r in range(TILES):
        lhs[:, r * LANES : (r + 1) * LANES] = wide[pl.ds(r, n, stride=TILES), :].astype(BF16)
    rows = lhs[...]
    gate = jnp.dot(rows, wg_ref[0], preferred_element_type=F32)
    up = jnp.dot(rows, wu_ref[0], preferred_element_type=F32)
    hidden = (jax.nn.silu(gate) * up).astype(BF16)
    out = jnp.dot(hidden, wd_ref[0], preferred_element_type=F32)
    for r in range(TILES):
        wide[pl.ds(r, n, stride=TILES), :] = out[:, r * LANES : (r + 1) * LANES]
    out_ref[...] = wide[...].astype(BF16).reshape(n, TILES, LANES)


def combine_kernel(group, inner, use, mixed_ref, back0_ref, back1_ref, out_ref, wide):
    for t in range(ROWS):
        total = mixed_ref[t].astype(F32)
        base = group[t] * PER_GROUP
        for j in range(2):
            e = base + inner[j, t]
            total = total + back0_ref[e].astype(F32) * use[0, j, t]
            total = total + back1_ref[e].astype(F32) * use[1, j, t]
        wide[t * TILES : (t + 1) * TILES, :] = total
    for r in range(TILES):
        out_ref[:, r * LANES : (r + 1) * LANES] = wide[
            pl.ds(r, ROWS, stride=TILES), :
        ].astype(BF16)


HBM = pl.BlockSpec(memory_space=pltpu.HBM)
VMEM = pl.BlockSpec(memory_space=pltpu.VMEM)
SMEM = pl.BlockSpec(memory_space=pltpu.SMEM)
ROW_TILES = (EXPERTS, TILES, LANES)


def local(
    tokens,
    history_length,
    norm_gain,
    w_query,
    w_key,
    w_value,
    w_gate,
    decay_rate,
    state,
    head_gain,
    w_out,
    moe_gain,
    route_weights,
    expert_group,
    expert_inner,
    expert_gate,
    expert_up,
    expert_down,
):
    inner = expert_inner.T
    inverse = jnp.asarray(
        (10000.0 ** (-(np.arange(LANES) % 32) / 32.0)).astype(np.float32).reshape(1, LANES)
    )
    mixed, send0, send1, keys, values = pl.pallas_call(
        front_kernel,
        out_shape=[
            jax.ShapeDtypeStruct((ROWS, TILES, LANES), BF16),
            jax.ShapeDtypeStruct(ROW_TILES, BF16),
            jax.ShapeDtypeStruct(ROW_TILES, BF16),
            jax.ShapeDtypeStruct((ROWS, RW), F32),
            jax.ShapeDtypeStruct((ROWS, RW), F32),
        ],
        in_specs=[HBM] * 15,
        out_specs=[VMEM] * 5,
        scratch_shapes=[
            pltpu.VMEM((1, ROWS), jnp.int32),
            pltpu.VMEM((1, LANES), F32),
            pltpu.VMEM((1, D), F32),
            pltpu.SMEM((HEADS,), F32),
            pltpu.VMEM((1, RW), F32),
            pltpu.VMEM((1, D), F32),
            pltpu.SMEM((ROWS,), jnp.int32),
            pltpu.SMEM((2, ROWS), jnp.int32),
            pltpu.VMEM((ROWS, D), BF16),
            pltpu.VMEM((4, D, RW), BF16),
            pltpu.VMEM((RW, D), BF16),
            pltpu.VMEM((ROWS, HEADS, HD, HD), F32),
            pltpu.VMEM((ROWS, RW), F32),
            pltpu.VMEM((HEADS * ROWS * 8, LANES), F32),
            pltpu.VMEM((ROWS * TILES, LANES), F32),
            pltpu.VMEM((ROWS, TILES, LANES), BF16),
            pltpu.SemaphoreType.DMA((9,)),
            pltpu.SemaphoreType.DMA((5,)),
            pltpu.SemaphoreType.DMA((CHUNKS,)),
        ],
        name="front",
    )(
        history_length.reshape(1, ROWS),
        inverse,
        norm_gain.reshape(1, D),
        decay_rate,
        head_gain.reshape(1, RW),
        moe_gain.reshape(1, D),
        expert_group,
        inner,
        tokens,
        w_query,
        w_key,
        w_value,
        w_gate,
        state,
        w_out,
    )
    new_state, use = pl.pallas_call(
        state_kernel,
        grid=(CHUNKS,),
        out_shape=[
            jax.ShapeDtypeStruct(state.shape, F32),
            jax.ShapeDtypeStruct((2, 2, ROWS), F32),
        ],
        in_specs=[
            SMEM,
            SMEM,
            SMEM,
            SMEM,
            pl.BlockSpec((GROUP, HEADS, HD, HD), lambda i: (i, 0, 0, 0)),
            pl.BlockSpec((GROUP, RW), lambda i: (i, 0)),
            pl.BlockSpec((GROUP, RW), lambda i: (i, 0)),
        ],
        out_specs=[
            pl.BlockSpec((GROUP, HEADS, HD, HD), lambda i: (i, 0, 0, 0)),
            SMEM,
        ],
        scratch_shapes=[pltpu.SMEM((EXPERTS,), jnp.int32)],
        cost_estimate=pl.CostEstimate(
            flops=10**9, bytes_accessed=26 * 10**6, transcendentals=0
        ),
        name="state_update",
    )(decay_rate, expert_group, inner, route_weights.T, state, keys, values)

    def dispatch(rows):
        return lax.all_to_all(rows, "ep", split_axis=0, concat_axis=0, tiled=True)

    expert = pl.pallas_call(
        expert_kernel,
        out_shape=jax.ShapeDtypeStruct(ROW_TILES, BF16),
        in_specs=[VMEM] * 4,
        out_specs=VMEM,
        scratch_shapes=[
            pltpu.VMEM((EXPERTS * TILES, LANES), F32),
            pltpu.VMEM((EXPERTS, D), BF16),
        ],
        cost_estimate=pl.CostEstimate(
            flops=4 * 10**8, bytes_accessed=4 * 10**6, transcendentals=0
        ),
        name="expert",
    )
    got0 = dispatch(send0)
    got1 = dispatch(send1)
    back0 = dispatch(expert(got0, expert_gate, expert_up, expert_down))
    back1 = dispatch(expert(got1, expert_gate, expert_up, expert_down))
    output = pl.pallas_call(
        combine_kernel,
        out_shape=jax.ShapeDtypeStruct((ROWS, D), BF16),
        in_specs=[SMEM, SMEM, SMEM, VMEM, VMEM, VMEM],
        out_specs=VMEM,
        scratch_shapes=[pltpu.VMEM((ROWS * TILES, LANES), F32)],
        name="combine",
    )(expert_group, inner, use, mixed, back0, back1)
    return output, new_state


def solution(mesh):
    return jax.shard_map(
        local,
        mesh=mesh,
        in_specs=(
            P("ep", None),
            P("ep"),
            P(),
            P(),
            P(),
            P(),
            P(),
            P(),
            P("ep", None, None, None),
            P(),
            P(),
            P(),
            P("ep", None),
            P("ep"),
            P("ep", None),
            P("ep", None, None),
            P("ep", None, None),
            P("ep", None, None),
        ),
        out_specs=(P("ep", None), P("ep", None, None, None)),
        check_vma=False,
    )
```

```python
import functools

import jax
import jax.numpy as jnp
import numpy as np
from jax import lax
from jax.experimental import pallas as pl
from jax.experimental.pallas import tpu as pltpu
from jax.sharding import PartitionSpec as P

EPS = 1e-06
ROWS = 48
D = 2048
HEADS = 8
HD = 64
RW = HEADS * HD
EXPERTS = 128
PER_GROUP = 32
LANES = 128
TILES = D // LANES
GROUP = 8
CHUNKS = ROWS // GROUP
F32 = jnp.float32
BF16 = jnp.bfloat16


def lane_iota(shape):
    return lax.broadcasted_iota(jnp.int32, shape, len(shape) - 1)


def group_sum(x, ones):
    high = x.astype(BF16)
    low = (x - high.astype(F32)).astype(BF16)
    return jnp.dot(high, ones, preferred_element_type=F32) + jnp.dot(
        low, ones, preferred_element_type=F32
    )


def rope(x, cosine, sine):
    lanes = lane_iota((ROWS, LANES))
    first = (lanes % HD) < (HD // 2)
    parts = []
    for c in range(RW // LANES):
        part = x[:, c * LANES : (c + 1) * LANES]
        other = jnp.where(
            first,
            pltpu.roll(part, LANES - HD // 2, 1),
            pltpu.roll(part, HD // 2, 1),
        )
        parts.append(part * cosine + other * jnp.where(first, -sine, sine))
    return jnp.concatenate(parts, axis=1)


def front_kernel(
    hist_hbm,
    inv_hbm,
    ngain_hbm,
    decay_hbm,
    hgain_hbm,
    mgain_hbm,
    group_hbm,
    inner_hbm,
    tok_hbm,
    wq_hbm,
    wk_hbm,
    wv_hbm,
    wg_hbm,
    state_hbm,
    wo_hbm,
    mixed_ref,
    send_ref,
    k_ref,
    v_ref,
    hist,
    inv,
    ngain,
    decay,
    hgain,
    mgain,
    group,
    inner,
    tok,
    w4,
    wo,
    st,
    qs,
    part,
    wide,
    tiles,
    small_sem,
    w_sem,
    st_sem,
):
    small = [
        pltpu.make_async_copy(tok_hbm, tok, small_sem.at[0]),
        pltpu.make_async_copy(ngain_hbm, ngain, small_sem.at[1]),
        pltpu.make_async_copy(hist_hbm, hist, small_sem.at[2]),
        pltpu.make_async_copy(inv_hbm, inv, small_sem.at[3]),
        pltpu.make_async_copy(decay_hbm, decay, small_sem.at[4]),
        pltpu.make_async_copy(hgain_hbm, hgain, small_sem.at[5]),
        pltpu.make_async_copy(mgain_hbm, mgain, small_sem.at[6]),
        pltpu.make_async_copy(group_hbm, group, small_sem.at[7]),
        pltpu.make_async_copy(inner_hbm, inner, small_sem.at[8]),
    ]
    for copy in small:
        copy.start()
    weights = [
        pltpu.make_async_copy(src, w4.at[i], w_sem.at[i])
        for i, src in enumerate((wq_hbm, wk_hbm, wv_hbm, wg_hbm))
    ]
    for copy in weights:
        copy.start()
    wo_copy = pltpu.make_async_copy(wo_hbm, wo, w_sem.at[4])
    wo_copy.start()
    states = [
        pltpu.make_async_copy(
            state_hbm.at[pl.ds(i * GROUP, GROUP)],
            st.at[pl.ds(i * GROUP, GROUP)],
            st_sem.at[i],
        )
        for i in range(CHUNKS)
    ]
    for copy in states:
        copy.start()
    for copy in small:
        copy.wait()

    x = tok[...].astype(F32)
    scale = lax.rsqrt(jnp.mean(x * x, axis=-1, keepdims=True) + EPS)
    normed = (x * scale * ngain[...]).astype(BF16)

    square = (ROWS, ROWS)
    place = jnp.sum(
        jnp.where(
            lax.broadcasted_iota(jnp.int32, square, 0) == lane_iota(square),
            jnp.broadcast_to(hist[...].astype(F32), square),
            0.0,
        ),
        axis=1,
        keepdims=True,
    )
    angles = place * inv[...]
    cosine = jnp.cos(angles)
    sine = jnp.sin(angles)

    zero = jnp.zeros((TILES, LANES), BF16)
    for e in range(2 * EXPERTS):
        send_ref[e] = zero

    def project(i):
        weights[i].wait()
        return jnp.dot(normed, w4[i], preferred_element_type=F32).astype(BF16).astype(F32)

    q = rope(project(0), cosine, sine)
    high = q.astype(BF16).astype(F32)
    qs[0] = high
    qs[1] = q - high
    k = rope(project(1), cosine, sine) * (HD**-0.5)
    k_ref[...] = k
    v = project(2)
    v_ref[...] = v
    gate = project(3)

    ones = (
        lax.broadcasted_iota(jnp.int32, (RW, RW), 0) // HD == lane_iota((RW, RW)) // HD
    ).astype(BF16)
    fresh = group_sum(q * k, ones) * v
    heads = lane_iota((1, RW)) // HD
    rate = jnp.zeros((1, RW), F32)
    for h in range(HEADS):
        rate = jnp.where(heads == h, decay[h], rate)
    retain = jnp.exp(-rate)

    own = (
        lax.broadcasted_iota(jnp.int32, (HEADS, RW), 0) == lane_iota((HEADS, RW)) // HD
    )

    def chunk(i, carry):
        pltpu.make_async_copy(
            state_hbm.at[pl.ds(i * GROUP, GROUP)],
            st.at[pl.ds(i * GROUP, GROUP)],
            st_sem.at[i],
        ).wait()
        for b in range(GROUP):
            t = i * GROUP + b
            spread = [
                jnp.where(own, jnp.broadcast_to(qs[s, pl.ds(t, 1), :], (HEADS, RW)), 0.0)
                for s in range(2)
            ]
            total = jnp.dot(
                jnp.concatenate(spread, axis=0).astype(BF16),
                st[t].reshape(RW, HD).astype(BF16),
                preferred_element_type=F32,
            )
            part[pl.ds(pl.multiple_of(t * HEADS, HEADS), HEADS), 0:HD] = (
                total[0:HEADS] + total[HEADS:]
            )
        return carry

    lax.fori_loop(0, CHUNKS, chunk, 0)

    def head_rows(h):
        return part[pl.ds(h, ROWS, stride=HEADS), :]

    low_half = lane_iota((ROWS, LANES)) < HD
    old = jnp.concatenate(
        [
            jnp.where(
                low_half, head_rows(2 * c), pltpu.roll(head_rows(2 * c + 1), HD, 1)
            )
            for c in range(HEADS // 2)
        ],
        axis=1,
    )
    reading = retain * old + fresh
    mean_square = group_sum(reading * reading, ones) * (1.0 / HD)
    reading = reading * lax.rsqrt(mean_square + EPS) * hgain[...]
    mixed_heads = (reading * jax.nn.silu(gate)).astype(BF16)
    wo_copy.wait()
    mixed = (x + jnp.dot(mixed_heads, wo[...], preferred_element_type=F32)).astype(BF16)
    mixed = mixed.astype(F32)
    scale = lax.rsqrt(jnp.mean(mixed * mixed, axis=-1, keepdims=True) + EPS)
    normed_moe = mixed * scale * mgain[...]

    for r in range(TILES):
        wide[pl.ds(r, ROWS, stride=TILES), :] = normed_moe[:, r * LANES : (r + 1) * LANES]
    tiles[...] = wide[...].astype(BF16).reshape(ROWS, TILES, LANES)
    for r in range(TILES):
        wide[pl.ds(r, ROWS, stride=TILES), :] = mixed[:, r * LANES : (r + 1) * LANES]
    mixed_ref[...] = wide[...].astype(BF16).reshape(ROWS, TILES, LANES)

    for t in range(ROWS):
        base = group[t] * PER_GROUP
        row = tiles[t]
        for j in range(2):
            send_ref[(base + inner[j, t]) * 2 + 1] = row
    for t in reversed(range(ROWS)):
        base = group[t] * PER_GROUP
        row = tiles[t]
        for j in (1, 0):
            send_ref[(base + inner[j, t]) * 2] = row


def state_kernel(decay, group, inner, state_ref, k_ref, v_ref, new_ref, slot_ref, seen):
    k = k_ref[...]
    high = k.astype(BF16).astype(F32)
    kt = jnp.concatenate([high, k - high], axis=0).T.astype(BF16)
    v = v_ref[...]
    swapped = jnp.concatenate(
        [
            pltpu.roll(v[:, c * LANES : (c + 1) * LANES], HD, 1)
            for c in range(RW // LANES)
        ],
        axis=1,
    )
    retains = [jnp.exp(jnp.full((HD, HD), -decay[h], F32)) for h in range(HEADS)]
    for pair in range(GROUP // 2):
        shape = (2 * GROUP, 2 * LANES)
        pick = (
            lax.broadcasted_iota(jnp.int32, shape, 0) % GROUP
            == lane_iota(shape) // LANES + 2 * pair
        ).astype(BF16)
        columns = jnp.dot(kt, pick, preferred_element_type=F32)
        for i in range(2):
            b = 2 * pair + i
            for h in range(HEADS):
                column = columns[h * HD : (h + 1) * HD, i * LANES : i * LANES + HD]
                c = (h // 2) * LANES
                row = (swapped if h % 2 else v)[b : b + 1, c : c + HD]
                new_ref[b, h] = retains[h] * state_ref[b, h] + column * row

    @pl.when(pl.program_id(0) == 0)
    def _():
        def clear(e, carry):
            seen[e] = 0
            return carry

        lax.fori_loop(0, EXPERTS, clear, 0)

        def visit(t, carry):
            for j in range(2):
                e = group[t] * PER_GROUP + inner[j, t]
                slot_ref[j, t] = 2 * e + seen[e]
                seen[e] = 1
            return carry

        lax.fori_loop(0, ROWS, visit, 0)


def expert_kernel(in_ref, wg_ref, wu_ref, wd_ref, out_ref, wide, lhs):
    n = in_ref.shape[0]
    wide[...] = in_ref[...].astype(F32).reshape(n * TILES, LANES)
    for r in range(TILES):
        lhs[:, r * LANES : (r + 1) * LANES] = wide[pl.ds(r, n, stride=TILES), :].astype(BF16)
    rows = lhs[...]
    gate = jnp.dot(rows, wg_ref[0], preferred_element_type=F32)
    up = jnp.dot(rows, wu_ref[0], preferred_element_type=F32)
    hidden = (jax.nn.silu(gate) * up).astype(BF16)
    out = jnp.dot(hidden, wd_ref[0], preferred_element_type=F32)
    for r in range(TILES):
        wide[pl.ds(r, n, stride=TILES), :] = out[:, r * LANES : (r + 1) * LANES]
    out_ref[...] = wide[...].astype(BF16).reshape(n, TILES, LANES)


def combine_kernel(slot, weight, mixed_ref, back_ref, out_ref, wide):
    for t in range(ROWS):
        total = mixed_ref[t].astype(F32)
        for j in range(2):
            total = total + back_ref[slot[j, t]].astype(F32) * weight[j, t]
        wide[t * TILES : (t + 1) * TILES, :] = total
    for r in range(TILES):
        out_ref[:, r * LANES : (r + 1) * LANES] = wide[
            pl.ds(r, ROWS, stride=TILES), :
        ].astype(BF16)


def in_vmem(x):
    return pltpu.with_memory_space_constraint(x, pltpu.VMEM)


def in_hbm(x):
    return pltpu.with_memory_space_constraint(x, pltpu.HBM)


HBM = pl.BlockSpec(memory_space=pltpu.HBM)
VMEM = pl.BlockSpec(memory_space=pltpu.VMEM)
SMEM = pl.BlockSpec(memory_space=pltpu.SMEM)
ROW_TILES = (2 * EXPERTS, TILES, LANES)


def local(
    tokens,
    history_length,
    norm_gain,
    w_query,
    w_key,
    w_value,
    w_gate,
    decay_rate,
    state,
    head_gain,
    w_out,
    moe_gain,
    route_weights,
    expert_group,
    expert_inner,
    expert_gate,
    expert_up,
    expert_down,
):
    inner = expert_inner.T
    inverse = jnp.asarray(
        (10000.0 ** (-(np.arange(LANES) % 32) / 32.0)).astype(np.float32).reshape(1, LANES)
    )
    mixed, send, keys, values = pl.pallas_call(
        front_kernel,
        out_shape=[
            pltpu.VMEM((ROWS, TILES, LANES), BF16),
            pltpu.VMEM(ROW_TILES, BF16),
            pltpu.VMEM((ROWS, RW), F32),
            pltpu.VMEM((ROWS, RW), F32),
        ],
        in_specs=[HBM] * 15,
        out_specs=[VMEM] * 4,
        scratch_shapes=[
            pltpu.VMEM((1, ROWS), jnp.int32),
            pltpu.VMEM((1, LANES), F32),
            pltpu.VMEM((1, D), F32),
            pltpu.SMEM((HEADS,), F32),
            pltpu.VMEM((1, RW), F32),
            pltpu.VMEM((1, D), F32),
            pltpu.SMEM((ROWS,), jnp.int32),
            pltpu.SMEM((2, ROWS), jnp.int32),
            pltpu.VMEM((ROWS, D), BF16),
            pltpu.VMEM((4, D, RW), BF16),
            pltpu.VMEM((RW, D), BF16),
            pltpu.VMEM((ROWS, HEADS, HD, HD), F32),
            pltpu.VMEM((2, ROWS, RW), F32),
            pltpu.VMEM((HEADS * ROWS, LANES), F32),
            pltpu.VMEM((ROWS * TILES, LANES), F32),
            pltpu.VMEM((ROWS, TILES, LANES), BF16),
            pltpu.SemaphoreType.DMA((9,)),
            pltpu.SemaphoreType.DMA((5,)),
            pltpu.SemaphoreType.DMA((CHUNKS,)),
        ],
        compiler_params=pltpu.CompilerParams(vmem_limit_bytes=36 * 2**20),
        name="front",
    )(
        *(
            in_hbm(x)
            for x in (
                history_length.reshape(1, ROWS),
                inverse,
                norm_gain.reshape(1, D),
                decay_rate,
                head_gain.reshape(1, RW),
                moe_gain.reshape(1, D),
                expert_group,
                inner,
                tokens,
                w_query,
                w_key,
                w_value,
                w_gate,
                state,
                w_out,
            )
        )
    )
    new_state, slots = pl.pallas_call(
        state_kernel,
        grid=(CHUNKS,),
        out_shape=[
            jax.ShapeDtypeStruct(state.shape, F32),
            jax.ShapeDtypeStruct((2, ROWS), jnp.int32),
        ],
        in_specs=[
            SMEM,
            SMEM,
            SMEM,
            pl.BlockSpec((GROUP, HEADS, HD, HD), lambda i: (i, 0, 0, 0)),
            pl.BlockSpec((GROUP, RW), lambda i: (i, 0)),
            pl.BlockSpec((GROUP, RW), lambda i: (i, 0)),
        ],
        out_specs=[
            pl.BlockSpec((GROUP, HEADS, HD, HD), lambda i: (i, 0, 0, 0)),
            SMEM,
        ],
        scratch_shapes=[pltpu.SMEM((EXPERTS,), jnp.int32)],
        cost_estimate=pl.CostEstimate(
            flops=10**9, bytes_accessed=26 * 10**6, transcendentals=0
        ),
        compiler_params=pltpu.CompilerParams(vmem_limit_bytes=20 * 2**20),
        name="state_update",
    )(
        in_hbm(decay_rate),
        in_hbm(expert_group),
        in_hbm(inner),
        in_hbm(state),
        in_vmem(keys),
        in_vmem(values),
    )

    def dispatch(rows):
        return lax.all_to_all(rows, "ep", split_axis=0, concat_axis=0, tiled=True)

    outputs = pl.pallas_call(
        expert_kernel,
        out_shape=pltpu.VMEM(ROW_TILES, BF16),
        in_specs=[VMEM] * 4,
        out_specs=VMEM,
        scratch_shapes=[
            pltpu.VMEM((2 * EXPERTS * TILES, LANES), F32),
            pltpu.VMEM((2 * EXPERTS, D), BF16),
        ],
        cost_estimate=pl.CostEstimate(
            flops=8 * 10**8, bytes_accessed=4 * 10**6, transcendentals=0
        ),
        compiler_params=pltpu.CompilerParams(vmem_limit_bytes=16 * 2**20),
        name="expert",
    )(
        in_vmem(dispatch(send)),
        in_vmem(expert_gate),
        in_vmem(expert_up),
        in_vmem(expert_down),
    )
    output = pl.pallas_call(
        combine_kernel,
        out_shape=jax.ShapeDtypeStruct((ROWS, D), BF16),
        in_specs=[SMEM, SMEM, VMEM, VMEM],
        out_specs=VMEM,
        scratch_shapes=[pltpu.VMEM((ROWS * TILES, LANES), F32)],
        compiler_params=pltpu.CompilerParams(vmem_limit_bytes=8 * 2**20),
        name="combine",
    )(slots, in_hbm(route_weights.T), in_vmem(mixed), in_vmem(dispatch(outputs)))
    return output, new_state


def solution(mesh):
    return jax.shard_map(
        local,
        mesh=mesh,
        in_specs=(
            P("ep", None),
            P("ep"),
            P(),
            P(),
            P(),
            P(),
            P(),
            P(),
            P("ep", None, None, None),
            P(),
            P(),
            P(),
            P("ep", None),
            P("ep"),
            P("ep", None),
            P("ep", None, None),
            P("ep", None, None),
            P("ep", None, None),
        ),
        out_specs=(P("ep", None), P("ep", None, None, None)),
        check_vma=False,
    )
```

```python
import functools

import jax
import jax.numpy as jnp
import numpy as np
from jax import lax
from jax.experimental import pallas as pl
from jax.experimental.pallas import tpu as pltpu
from jax.sharding import PartitionSpec as P

EPS = 1e-06
ROWS = 48
D = 2048
HEADS = 8
HD = 64
RW = HEADS * HD
EXPERTS = 128
PER_GROUP = 32
LANES = 128
TILES = D // LANES
GROUP = 8
CHUNKS = ROWS // GROUP
BLOCK = 128
PART = 16
F32 = jnp.float32
BF16 = jnp.bfloat16


def lane_iota(shape):
    return lax.broadcasted_iota(jnp.int32, shape, len(shape) - 1)


def row_iota(shape):
    return lax.broadcasted_iota(jnp.int32, shape, 0)


def split(x):
    high = x.astype(BF16).astype(F32)
    return high, x - high


def by_lanes(f, x):
    return jnp.concatenate(
        [f(x[:, c * LANES : (c + 1) * LANES]) for c in range(x.shape[1] // LANES)],
        axis=1,
    )


def head_sum(x):
    shape = (LANES, LANES)
    ones = (row_iota(shape) // HD == lane_iota(shape) // HD).astype(BF16)

    def part(y):
        high, low = split(y)
        return jnp.dot(high.astype(BF16), ones, preferred_element_type=F32) + jnp.dot(
            low.astype(BF16), ones, preferred_element_type=F32
        )

    return by_lanes(part, x)


def rope(x, cosine, sine):
    first = (lane_iota((ROWS, LANES)) % HD) < (HD // 2)

    def part(y):
        other = jnp.where(
            first, pltpu.roll(y, LANES - HD // 2, 1), pltpu.roll(y, HD // 2, 1)
        )
        return y * cosine + other * sine

    return by_lanes(part, x)


def front_kernel(
    hist_hbm,
    inv_hbm,
    ngain_hbm,
    decay_hbm,
    hgain_hbm,
    mgain_hbm,
    group_hbm,
    inner_hbm,
    weight_hbm,
    tok_hbm,
    wq_hbm,
    wk_hbm,
    wv_hbm,
    wg_hbm,
    state_hbm,
    wo_hbm,
    mixed_ref,
    send_ref,
    k_ref,
    v_ref,
    slot_ref,
    weight_ref,
    hist,
    inv,
    ngain,
    decay,
    hgain,
    mgain,
    group,
    inner,
    seen,
    tok,
    w4,
    wo,
    st,
    qs,
    part,
    wide,
    scales,
    small_sem,
    w_sem,
    st_sem,
):
    small = [
        pltpu.make_async_copy(src, dst, small_sem.at[i])
        for i, (src, dst) in enumerate(
            (
                (tok_hbm, tok),
                (ngain_hbm, ngain),
                (hist_hbm, hist),
                (inv_hbm, inv),
                (decay_hbm, decay),
                (hgain_hbm, hgain),
                (mgain_hbm, mgain),
                (group_hbm, group),
                (inner_hbm, inner),
                (weight_hbm, weight_ref),
            )
        )
    ]
    weights = [
        pltpu.make_async_copy(src, w4.at[i], w_sem.at[i])
        for i, src in enumerate((wq_hbm, wk_hbm, wv_hbm, wg_hbm))
    ]
    wo_copy = pltpu.make_async_copy(wo_hbm, wo, w_sem.at[4])

    def state_copy(i):
        rows = pl.ds(i * GROUP, GROUP)
        return pltpu.make_async_copy(state_hbm.at[rows], st.at[rows], st_sem.at[i])

    for copy in small:
        copy.start()
    for copy in weights:
        copy.start()
    for copy in small:
        copy.wait()
    state_copy(0).start()

    x = tok[...].astype(F32)
    scale = lax.rsqrt(jnp.mean(x * x, axis=-1, keepdims=True) + EPS)
    normed = (x * scale * ngain[...]).astype(BF16)

    square = (ROWS, ROWS)
    place = jnp.sum(
        jnp.where(
            row_iota(square) == lane_iota(square),
            jnp.broadcast_to(hist[...].astype(F32), square),
            0.0,
        ),
        axis=1,
        keepdims=True,
    )
    angles = place * inv[...]
    cosine = jnp.cos(angles)
    sine = jnp.sin(angles)
    sine = jnp.where((lane_iota((ROWS, LANES)) % HD) < (HD // 2), -sine, sine)

    for e in range(EXPERTS):
        seen[e] = 0
    for t in range(ROWS):
        for j in range(2):
            e = group[t] * PER_GROUP + inner[j, t]
            slot = seen[e]
            seen[e] = 1
            slot_ref[j, t] = 2 * e + slot
    zero = jnp.zeros((TILES, LANES), BF16)
    for e in range(2 * EXPERTS):
        send_ref[e] = zero

    def project(i):
        weights[i].wait()
        return jnp.dot(normed, w4[i], preferred_element_type=F32).astype(BF16).astype(F32)

    q = project(0)
    for i in range(1, 3):
        state_copy(i).start()
    q = rope(q, cosine, sine)
    k = project(1)
    for i in range(3, CHUNKS):
        state_copy(i).start()
    wo_copy.start()
    k = rope(k, cosine, sine) * (HD**-0.5)
    v = project(2)
    gate = project(3)
    for i, piece in enumerate(split(q)):
        qs[i] = piece
    k_ref[...] = k
    v_ref[...] = v

    fresh = head_sum(q * k) * v
    heads = lane_iota((1, RW)) // HD
    rate = jnp.zeros((1, RW), F32)
    for h in range(HEADS):
        rate = jnp.where(heads == h, decay[h], rate)
    retain = jnp.exp(-rate)
    own = row_iota((HEADS, RW)) == lane_iota((HEADS, RW)) // HD

    def read(t):
        spread = [
            jnp.where(own, jnp.broadcast_to(qs[s, pl.ds(t, 1), :], (HEADS, RW)), 0.0)
            for s in range(2)
        ]
        total = jnp.dot(
            jnp.concatenate(spread, axis=0).astype(BF16),
            st[t].reshape(RW, HD).astype(BF16),
            preferred_element_type=F32,
        )
        part[pl.ds(pl.multiple_of(t * HEADS, HEADS), HEADS), 0:HD] = (
            total[0:HEADS] + total[HEADS:]
        )

    def chunk(i, carry):
        state_copy(i).wait()
        for b in range(GROUP):
            read(i * GROUP + b)
        return carry

    lax.fori_loop(0, CHUNKS, chunk, 0)

    def head_rows(h):
        return part[pl.ds(h, ROWS, stride=HEADS), :]

    low_half = lane_iota((ROWS, LANES)) < HD
    old = jnp.concatenate(
        [
            jnp.where(
                low_half, head_rows(2 * c), pltpu.roll(head_rows(2 * c + 1), HD, 1)
            )
            for c in range(HEADS // 2)
        ],
        axis=1,
    )
    reading = retain * old + fresh
    mean_square = head_sum(reading * reading) * (1.0 / HD)
    reading = reading * lax.rsqrt(mean_square + EPS) * hgain[...]
    mixed_heads = (reading * jax.nn.silu(gate)).astype(BF16)
    wo_copy.wait()
    squares = jnp.zeros((ROWS, LANES), F32)
    for n in range(0, D, 2 * LANES):
        block = slice(n, n + 2 * LANES)
        mixed = tok[:, block].astype(F32) + jnp.dot(
            mixed_heads, wo[:, block], preferred_element_type=F32
        )
        mixed = mixed.astype(BF16).astype(F32)
        for i in range(2):
            piece = mixed[:, i * LANES : (i + 1) * LANES]
            squares = squares + piece * piece
            wide[pl.ds(n // LANES + i, ROWS, stride=TILES), :] = piece
    scale = lax.rsqrt(jnp.sum(squares, axis=-1, keepdims=True) * (1.0 / D) + EPS)
    scales[...] = jnp.broadcast_to(scale, (ROWS, LANES))
    for t in range(ROWS):
        tile = wide[t * TILES : (t + 1) * TILES, :]
        mixed_ref[t] = tile.astype(BF16)
        row = (tile * scales[t : t + 1, :] * mgain[...]).astype(BF16)
        for j in range(2):
            send_ref[slot_ref[j, t]] = row


def state_kernel(decay, state_ref, k_ref, v_ref, new_ref):
    k = k_ref[...]
    high = k.astype(BF16).astype(F32)
    kt = jnp.concatenate([high, k - high], axis=0).T.astype(BF16)
    v = v_ref[...]
    swapped = jnp.concatenate(
        [
            pltpu.roll(v[:, c * LANES : (c + 1) * LANES], HD, 1)
            for c in range(RW // LANES)
        ],
        axis=1,
    )
    retains = [jnp.exp(jnp.full((HD, HD), -decay[h], F32)) for h in range(HEADS)]
    for pair in range(GROUP // 2):
        shape = (2 * GROUP, 2 * LANES)
        pick = (
            lax.broadcasted_iota(jnp.int32, shape, 0) % GROUP
            == lane_iota(shape) // LANES + 2 * pair
        ).astype(BF16)
        columns = jnp.dot(kt, pick, preferred_element_type=F32)
        for i in range(2):
            b = 2 * pair + i
            for h in range(HEADS):
                column = columns[h * HD : (h + 1) * HD, i * LANES : i * LANES + HD]
                c = (h // 2) * LANES
                row = (swapped if h % 2 else v)[b : b + 1, c : c + HD]
                new_ref[b, h] = retains[h] * state_ref[b, h] + column * row


def expert_kernel(
    in_ref, wg_ref, wu_ref, wd_hbm, out_hbm, wide, lhs, out, down, sem, down_sem
):
    down_copy = pltpu.make_async_copy(wd_hbm, down, down_sem)
    down_copy.start()
    copies = []
    for i in range(2 * EXPERTS // BLOCK):
        rows = pl.ds(i * BLOCK, BLOCK)
        wide[i] = in_ref[rows].astype(F32).reshape(BLOCK * TILES, LANES)
        for r in range(TILES):
            lhs[rows, r * LANES : (r + 1) * LANES] = wide[
                i, pl.ds(r, BLOCK, stride=TILES), :
            ].astype(BF16)
        gate = jnp.dot(lhs[rows], wg_ref[0], preferred_element_type=F32)
        up = jnp.dot(lhs[rows], wu_ref[0], preferred_element_type=F32)
        hidden = (jax.nn.silu(gate) * up).astype(BF16)
        if i == 0:
            down_copy.wait()
        result = jnp.dot(hidden, down[0], preferred_element_type=F32)
        for r in range(TILES):
            wide[i, pl.ds(r, BLOCK, stride=TILES), :] = result[
                :, r * LANES : (r + 1) * LANES
            ]
        out[rows] = wide[i].astype(BF16).reshape(BLOCK, TILES, LANES)
        copy = pltpu.make_async_copy(out.at[rows], out_hbm.at[rows], sem.at[i])
        copy.start()
        copies.append(copy)
    for copy in copies:
        copy.wait()


def combine_kernel(slot, weight, mixed_ref, back_ref, out_hbm, wide, out, sem):
    copies = []
    for i in range(ROWS // PART):
        for t in range(i * PART, (i + 1) * PART):
            total = mixed_ref[t].astype(F32)
            for j in range(2):
                total = total + back_ref[slot[j, t]].astype(F32) * weight[j, t]
            wide[t * TILES : (t + 1) * TILES, :] = total
        rows = pl.ds(i * PART, PART)
        for r in range(TILES):
            out[rows, r * LANES : (r + 1) * LANES] = wide[
                pl.ds(i * PART * TILES + r, PART, stride=TILES), :
            ].astype(BF16)
        copy = pltpu.make_async_copy(out.at[rows], out_hbm.at[rows], sem.at[i])
        copy.start()
        copies.append(copy)
    for copy in copies:
        copy.wait()


def in_vmem(x):
    return pltpu.with_memory_space_constraint(x, pltpu.VMEM)


def in_smem(x):
    return pltpu.with_memory_space_constraint(x, pltpu.SMEM)


def in_hbm(x):
    return pltpu.with_memory_space_constraint(x, pltpu.HBM)


HBM = pl.BlockSpec(memory_space=pltpu.HBM)
VMEM = pl.BlockSpec(memory_space=pltpu.VMEM)
SMEM = pl.BlockSpec(memory_space=pltpu.SMEM)
ROW_TILES = (2 * EXPERTS, TILES, LANES)


def local(
    tokens,
    history_length,
    norm_gain,
    w_query,
    w_key,
    w_value,
    w_gate,
    decay_rate,
    state,
    head_gain,
    w_out,
    moe_gain,
    route_weights,
    expert_group,
    expert_inner,
    expert_gate,
    expert_up,
    expert_down,
):
    inner = expert_inner.T
    inverse = jnp.asarray(
        (10000.0 ** (-(np.arange(LANES) % 32) / 32.0)).astype(np.float32).reshape(1, LANES)
    )
    mixed, send, keys, values, slots, weights = pl.pallas_call(
        front_kernel,
        out_shape=[
            pltpu.VMEM((ROWS, TILES, LANES), BF16),
            pltpu.VMEM(ROW_TILES, BF16),
            pltpu.VMEM((ROWS, RW), F32),
            pltpu.VMEM((ROWS, RW), F32),
            pltpu.SMEM((2, ROWS), jnp.int32),
            pltpu.SMEM((2, ROWS), F32),
        ],
        in_specs=[HBM] * 16,
        out_specs=[VMEM, VMEM, VMEM, VMEM, SMEM, SMEM],
        scratch_shapes=[
            pltpu.VMEM((1, ROWS), jnp.int32),
            pltpu.VMEM((1, LANES), F32),
            pltpu.VMEM((1, D), F32),
            pltpu.SMEM((HEADS,), F32),
            pltpu.VMEM((1, RW), F32),
            pltpu.VMEM((TILES, LANES), F32),
            pltpu.SMEM((ROWS,), jnp.int32),
            pltpu.SMEM((2, ROWS), jnp.int32),
            pltpu.SMEM((EXPERTS,), jnp.int32),
            pltpu.VMEM((ROWS, D), BF16),
            pltpu.VMEM((4, D, RW), BF16),
            pltpu.VMEM((RW, D), BF16),
            pltpu.VMEM((ROWS, HEADS, HD, HD), F32),
            pltpu.VMEM((2, ROWS, RW), F32),
            pltpu.VMEM((HEADS * ROWS, LANES), F32),
            pltpu.VMEM((ROWS * TILES, LANES), F32),
            pltpu.VMEM((ROWS, LANES), F32),
            pltpu.SemaphoreType.DMA((10,)),
            pltpu.SemaphoreType.DMA((5,)),
            pltpu.SemaphoreType.DMA((CHUNKS,)),
        ],
        compiler_params=pltpu.CompilerParams(vmem_limit_bytes=32 * 2**20),
        name="front",
    )(
        *(
            in_hbm(x)
            for x in (
                history_length.reshape(1, ROWS),
                inverse,
                norm_gain.reshape(1, D),
                decay_rate,
                head_gain.reshape(1, RW),
                moe_gain.reshape(TILES, LANES),
                expert_group,
                inner,
                route_weights.T,
                tokens,
                w_query,
                w_key,
                w_value,
                w_gate,
                state,
                w_out,
            )
        )
    )

    new_state = pl.pallas_call(
        state_kernel,
        grid=(CHUNKS,),
        out_shape=jax.ShapeDtypeStruct(state.shape, F32),
        in_specs=[
            SMEM,
            pl.BlockSpec((GROUP, HEADS, HD, HD), lambda i: (i, 0, 0, 0)),
            pl.BlockSpec((GROUP, RW), lambda i: (i, 0)),
            pl.BlockSpec((GROUP, RW), lambda i: (i, 0)),
        ],
        out_specs=pl.BlockSpec((GROUP, HEADS, HD, HD), lambda i: (i, 0, 0, 0)),
        cost_estimate=pl.CostEstimate(
            flops=10**9, bytes_accessed=26 * 10**6, transcendentals=0
        ),
        compiler_params=pltpu.CompilerParams(vmem_limit_bytes=20 * 2**20),
        name="state_update",
    )(in_hbm(decay_rate), in_hbm(state), in_vmem(keys), in_vmem(values))

    def dispatch(rows):
        return lax.all_to_all(rows, "ep", split_axis=0, concat_axis=0, tiled=True)

    outputs = pl.pallas_call(
        expert_kernel,
        out_shape=jax.ShapeDtypeStruct(ROW_TILES, BF16),
        in_specs=[VMEM, VMEM, VMEM, HBM],
        out_specs=HBM,
        scratch_shapes=[
            pltpu.VMEM((2 * EXPERTS // BLOCK, BLOCK * TILES, LANES), F32),
            pltpu.VMEM((2 * EXPERTS, D), BF16),
            pltpu.VMEM(ROW_TILES, BF16),
            pltpu.VMEM((1, RW // 2, D), BF16),
            pltpu.SemaphoreType.DMA((2 * EXPERTS // BLOCK,)),
            pltpu.SemaphoreType.DMA,
        ],
        cost_estimate=pl.CostEstimate(
            flops=8 * 10**8, bytes_accessed=4 * 10**6, transcendentals=0
        ),
        compiler_params=pltpu.CompilerParams(vmem_limit_bytes=16 * 2**20),
        name="expert",
    )(
        in_vmem(dispatch(send)),
        in_vmem(expert_gate),
        in_vmem(expert_up),
        in_hbm(expert_down),
    )
    output = pl.pallas_call(
        combine_kernel,
        out_shape=jax.ShapeDtypeStruct((ROWS, D), BF16),
        in_specs=[SMEM, SMEM, VMEM, VMEM],
        out_specs=HBM,
        scratch_shapes=[
            pltpu.VMEM((ROWS * TILES, LANES), F32),
            pltpu.VMEM((ROWS, D), BF16),
            pltpu.SemaphoreType.DMA((ROWS // PART,)),
        ],
        compiler_params=pltpu.CompilerParams(vmem_limit_bytes=8 * 2**20),
        name="combine",
    )(in_smem(slots), in_smem(weights), in_vmem(mixed), in_vmem(dispatch(outputs)))
    return output, new_state


def solution(mesh):
    return jax.shard_map(
        local,
        mesh=mesh,
        in_specs=(
            P("ep", None),
            P("ep"),
            P(),
            P(),
            P(),
            P(),
            P(),
            P(),
            P("ep", None, None, None),
            P(),
            P(),
            P(),
            P("ep", None),
            P("ep"),
            P("ep", None),
            P("ep", None, None),
            P("ep", None, None),
            P("ep", None, None),
        ),
        out_specs=(P("ep", None), P("ep", None, None, None)),
        check_vma=False,
    )
```

```python
import functools

import jax
import jax.numpy as jnp
import numpy as np
from jax import lax
from jax.experimental import pallas as pl
from jax.experimental.pallas import tpu as pltpu
from jax.sharding import PartitionSpec as P

EPS = 1e-06
ROWS = 48
D = 2048
HEADS = 8
HD = 64
RW = HEADS * HD
EXPERTS = 128
PER_GROUP = 32
LANES = 128
TILES = D // LANES
GROUP = 8
CHUNKS = ROWS // GROUP
STEP = 20
PART = 16
COPIES = 4
F32 = jnp.float32
BF16 = jnp.bfloat16


def lane_iota(shape):
    return lax.broadcasted_iota(jnp.int32, shape, len(shape) - 1)


def row_iota(shape):
    return lax.broadcasted_iota(jnp.int32, shape, 0)


def split(x):
    high = x.astype(BF16).astype(F32)
    return high, x - high


def by_lanes(f, x):
    return jnp.concatenate(
        [f(x[:, c * LANES : (c + 1) * LANES]) for c in range(x.shape[1] // LANES)],
        axis=1,
    )


def head_sum(x):
    shape = (LANES, LANES)
    ones = (row_iota(shape) // HD == lane_iota(shape) // HD).astype(BF16)

    def part(y):
        high, low = split(y)
        return jnp.dot(high.astype(BF16), ones, preferred_element_type=F32) + jnp.dot(
            low.astype(BF16), ones, preferred_element_type=F32
        )

    return by_lanes(part, x)


def rope(x, cosine, sine):
    first = (lane_iota((ROWS, LANES)) % HD) < (HD // 2)

    def part(y):
        other = jnp.where(
            first, pltpu.roll(y, LANES - HD // 2, 1), pltpu.roll(y, HD // 2, 1)
        )
        return y * cosine + other * sine

    return by_lanes(part, x)


def front_kernel(
    hist_hbm,
    inv_hbm,
    ngain_hbm,
    decay_hbm,
    hgain_hbm,
    mgain_hbm,
    group_hbm,
    inner_hbm,
    weight_hbm,
    tok_hbm,
    wq_hbm,
    wk_hbm,
    wv_hbm,
    wg_hbm,
    state_hbm,
    wo_hbm,
    down_hbm,
    mixed_ref,
    send_ref,
    k_ref,
    v_ref,
    slot_ref,
    weight_ref,
    down_ref,
    hist,
    inv,
    ngain,
    decay,
    hgain,
    mgain,
    group,
    inner,
    seen,
    tok,
    w4,
    wo,
    st,
    qs,
    part,
    wide,
    scales,
    small_sem,
    w_sem,
    st_sem,
):
    small = [
        pltpu.make_async_copy(src, dst, small_sem.at[i])
        for i, (src, dst) in enumerate(
            (
                (tok_hbm, tok),
                (ngain_hbm, ngain),
                (hist_hbm, hist),
                (inv_hbm, inv),
                (decay_hbm, decay),
                (hgain_hbm, hgain),
                (mgain_hbm, mgain),
                (group_hbm, group),
                (inner_hbm, inner),
                (weight_hbm, weight_ref),
            )
        )
    ]
    weights = [
        pltpu.make_async_copy(src, w4.at[i], w_sem.at[i])
        for i, src in enumerate((wq_hbm, wk_hbm, wv_hbm, wg_hbm))
    ]
    wo_copy = pltpu.make_async_copy(wo_hbm, wo, w_sem.at[4])
    down_copy = pltpu.make_async_copy(down_hbm, down_ref, w_sem.at[5])

    def state_copy(i):
        rows = pl.ds(i * GROUP, GROUP)
        return pltpu.make_async_copy(state_hbm.at[rows], st.at[rows], st_sem.at[i])

    for copy in small:
        copy.start()
    for copy in weights:
        copy.start()
    for copy in small:
        copy.wait()
    state_copy(0).start()

    x = tok[...].astype(F32)
    scale = lax.rsqrt(jnp.mean(x * x, axis=-1, keepdims=True) + EPS)
    normed = (x * scale * ngain[...]).astype(BF16)

    square = (ROWS, ROWS)
    place = jnp.sum(
        jnp.where(
            row_iota(square) == lane_iota(square),
            jnp.broadcast_to(hist[...].astype(F32), square),
            0.0,
        ),
        axis=1,
        keepdims=True,
    )
    angles = place * inv[...]
    cosine = jnp.cos(angles)
    sine = jnp.sin(angles)
    sine = jnp.where((lane_iota((ROWS, LANES)) % HD) < (HD // 2), -sine, sine)

    for e in range(EXPERTS):
        seen[e] = 0
    for t in range(ROWS):
        for j in range(2):
            e = group[t] * PER_GROUP + inner[j, t]
            slot = seen[e]
            seen[e] = 1
            slot_ref[j, t] = 2 * e + slot
    zero = jnp.zeros((TILES, LANES), BF16)
    for e in range(2 * EXPERTS):
        send_ref[e] = zero

    def project(i):
        weights[i].wait()
        return jnp.dot(normed, w4[i], preferred_element_type=F32).astype(BF16).astype(F32)

    q = project(0)
    for i in range(1, 3):
        state_copy(i).start()
    q = rope(q, cosine, sine)
    k = project(1)
    for i in range(3, CHUNKS):
        state_copy(i).start()
    wo_copy.start()
    k = rope(k, cosine, sine) * (HD**-0.5)
    v = project(2)
    down_copy.start()
    gate = project(3)
    for i, piece in enumerate(split(q)):
        qs[i] = piece
    k_ref[...] = k
    v_ref[...] = v

    fresh = head_sum(q * k) * v
    heads = lane_iota((1, RW)) // HD
    rate = jnp.zeros((1, RW), F32)
    for h in range(HEADS):
        rate = jnp.where(heads == h, decay[h], rate)
    retain = jnp.exp(-rate)
    own = row_iota((HEADS, RW)) == lane_iota((HEADS, RW)) // HD

    def read(t):
        spread = [
            jnp.where(own, jnp.broadcast_to(qs[s, pl.ds(t, 1), :], (HEADS, RW)), 0.0)
            for s in range(2)
        ]
        total = jnp.dot(
            jnp.concatenate(spread, axis=0).astype(BF16),
            st[t].reshape(RW, HD).astype(BF16),
            preferred_element_type=F32,
        )
        part[pl.ds(t * (HEADS + 1), HEADS), 0:HD] = (
            total[0:HEADS] + total[HEADS:]
        )

    def chunk(i, carry):
        state_copy(i).wait()
        for b in range(GROUP):
            read(i * GROUP + b)
        return carry

    lax.fori_loop(0, CHUNKS, chunk, 0)

    def head_rows(h):
        return part[pl.ds(h, ROWS, stride=HEADS + 1), :]

    low_half = lane_iota((ROWS, LANES)) < HD
    old = jnp.concatenate(
        [
            jnp.where(
                low_half, head_rows(2 * c), pltpu.roll(head_rows(2 * c + 1), HD, 1)
            )
            for c in range(HEADS // 2)
        ],
        axis=1,
    )
    reading = retain * old + fresh
    mean_square = head_sum(reading * reading) * (1.0 / HD)
    reading = reading * lax.rsqrt(mean_square + EPS) * hgain[...]
    mixed_heads = (reading * jax.nn.silu(gate)).astype(BF16)
    wo_copy.wait()
    squares = jnp.zeros((ROWS, LANES), F32)
    for n in range(0, D, 2 * LANES):
        block = slice(n, n + 2 * LANES)
        mixed = tok[:, block].astype(F32) + jnp.dot(
            mixed_heads, wo[:, block], preferred_element_type=F32
        )
        mixed = mixed.astype(BF16).astype(F32)
        for i in range(2):
            piece = mixed[:, i * LANES : (i + 1) * LANES]
            squares = squares + piece * piece
            wide[pl.ds(n // LANES + i, ROWS, stride=STEP), :] = piece
    scale = lax.rsqrt(jnp.sum(squares, axis=-1, keepdims=True) * (1.0 / D) + EPS)
    scales[...] = jnp.broadcast_to(scale, (ROWS, LANES))
    for t in range(ROWS):
        tile = wide[t * STEP : t * STEP + TILES, :]
        mixed_ref[t] = tile.astype(BF16)
        row = (tile * scales[t : t + 1, :] * mgain[...]).astype(BF16)
        for j in range(2):
            send_ref[slot_ref[j, t]] = row
    down_copy.wait()


def state_kernel(decay, state_ref, k_ref, v_ref, new_ref):
    k = k_ref[...]
    high = k.astype(BF16).astype(F32)
    kt = jnp.concatenate([high, k - high], axis=0).T.astype(BF16)
    v = v_ref[...]
    swapped = jnp.concatenate(
        [
            pltpu.roll(v[:, c * LANES : (c + 1) * LANES], HD, 1)
            for c in range(RW // LANES)
        ],
        axis=1,
    )
    retains = [jnp.exp(jnp.full((HD, HD), -decay[h], F32)) for h in range(HEADS)]
    for pair in range(GROUP // 2):
        shape = (2 * GROUP, 2 * LANES)
        pick = (
            lax.broadcasted_iota(jnp.int32, shape, 0) % GROUP
            == lane_iota(shape) // LANES + 2 * pair
        ).astype(BF16)
        columns = jnp.dot(kt, pick, preferred_element_type=F32)
        for i in range(2):
            b = 2 * pair + i
            for h in range(HEADS):
                column = columns[h * HD : (h + 1) * HD, i * LANES : i * LANES + HD]
                c = (h // 2) * LANES
                row = (swapped if h % 2 else v)[b : b + 1, c : c + HD]
                new_ref[b, h] = retains[h] * state_ref[b, h] + column * row


def expert_kernel(in_ref, wg_ref, wu_ref, wd_ref, out_hbm, wide, lhs, out, sem):
    n = 2 * EXPERTS
    for i in range(n):
        wide[i * STEP : i * STEP + TILES, :] = in_ref[i].astype(F32)
    for r in range(TILES):
        lhs[:, r * LANES : (r + 1) * LANES] = wide[pl.ds(r, n, stride=STEP), :].astype(BF16)
    rows = lhs[...]
    gate = jnp.dot(rows, wg_ref[0], preferred_element_type=F32)
    up = jnp.dot(rows, wu_ref[0], preferred_element_type=F32)
    hidden = (jax.nn.silu(gate) * up).astype(BF16)
    result = jnp.dot(hidden, wd_ref[0], preferred_element_type=F32)
    for r in range(TILES):
        wide[pl.ds(r, n, stride=STEP), :] = result[:, r * LANES : (r + 1) * LANES]
    copies = []
    for c in range(COPIES):
        for i in range(c * n // COPIES, (c + 1) * n // COPIES):
            out[i] = wide[i * STEP : i * STEP + TILES, :].astype(BF16)
        rows = pl.ds(c * n // COPIES, n // COPIES)
        copy = pltpu.make_async_copy(out.at[rows], out_hbm.at[rows], sem.at[c])
        copy.start()
        copies.append(copy)
    for copy in copies:
        copy.wait()


def combine_kernel(slot, weight, mixed_ref, back_ref, out_hbm, wide, out, sem):
    copies = []
    for i in range(ROWS // PART):
        for t in range(i * PART, (i + 1) * PART):
            total = mixed_ref[t].astype(F32)
            for j in range(2):
                total = total + back_ref[slot[j, t]].astype(F32) * weight[j, t]
            wide[t * STEP : t * STEP + TILES, :] = total
        rows = pl.ds(i * PART, PART)
        for r in range(TILES):
            out[rows, r * LANES : (r + 1) * LANES] = wide[
                pl.ds(i * PART * STEP + r, PART, stride=STEP), :
            ].astype(BF16)
        copy = pltpu.make_async_copy(out.at[rows], out_hbm.at[rows], sem.at[i])
        copy.start()
        copies.append(copy)
    for copy in copies:
        copy.wait()


def in_vmem(x):
    return pltpu.with_memory_space_constraint(x, pltpu.VMEM)


def in_smem(x):
    return pltpu.with_memory_space_constraint(x, pltpu.SMEM)


def in_hbm(x):
    return pltpu.with_memory_space_constraint(x, pltpu.HBM)


HBM = pl.BlockSpec(memory_space=pltpu.HBM)
VMEM = pl.BlockSpec(memory_space=pltpu.VMEM)
SMEM = pl.BlockSpec(memory_space=pltpu.SMEM)
ROW_TILES = (2 * EXPERTS, TILES, LANES)


def local(
    tokens,
    history_length,
    norm_gain,
    w_query,
    w_key,
    w_value,
    w_gate,
    decay_rate,
    state,
    head_gain,
    w_out,
    moe_gain,
    route_weights,
    expert_group,
    expert_inner,
    expert_gate,
    expert_up,
    expert_down,
):
    inner = expert_inner.T
    inverse = jnp.asarray(
        (10000.0 ** (-(np.arange(LANES) % 32) / 32.0)).astype(np.float32).reshape(1, LANES)
    )
    mixed, send, keys, values, slots, weights, down = pl.pallas_call(
        front_kernel,
        out_shape=[
            pltpu.VMEM((ROWS, TILES, LANES), BF16),
            pltpu.VMEM(ROW_TILES, BF16),
            pltpu.VMEM((ROWS, RW), F32),
            pltpu.VMEM((ROWS, RW), F32),
            pltpu.SMEM((2, ROWS), jnp.int32),
            pltpu.SMEM((2, ROWS), F32),
            pltpu.VMEM(expert_down.shape, BF16),
        ],
        in_specs=[HBM] * 17,
        out_specs=[VMEM, VMEM, VMEM, VMEM, SMEM, SMEM, VMEM],
        scratch_shapes=[
            pltpu.VMEM((1, ROWS), jnp.int32),
            pltpu.VMEM((1, LANES), F32),
            pltpu.VMEM((1, D), F32),
            pltpu.SMEM((HEADS,), F32),
            pltpu.VMEM((1, RW), F32),
            pltpu.VMEM((TILES, LANES), F32),
            pltpu.SMEM((ROWS,), jnp.int32),
            pltpu.SMEM((2, ROWS), jnp.int32),
            pltpu.SMEM((EXPERTS,), jnp.int32),
            pltpu.VMEM((ROWS, D), BF16),
            pltpu.VMEM((4, D, RW), BF16),
            pltpu.VMEM((RW, D), BF16),
            pltpu.VMEM((ROWS, HEADS, HD, HD), F32),
            pltpu.VMEM((2, ROWS, RW), F32),
            pltpu.VMEM(((HEADS + 1) * ROWS, LANES), F32),
            pltpu.VMEM((ROWS * STEP, LANES), F32),
            pltpu.VMEM((ROWS, LANES), F32),
            pltpu.SemaphoreType.DMA((10,)),
            pltpu.SemaphoreType.DMA((6,)),
            pltpu.SemaphoreType.DMA((CHUNKS,)),
        ],
        compiler_params=pltpu.CompilerParams(vmem_limit_bytes=32 * 2**20),
        name="front",
    )(
        *(
            in_hbm(x)
            for x in (
                history_length.reshape(1, ROWS),
                inverse,
                norm_gain.reshape(1, D),
                decay_rate,
                head_gain.reshape(1, RW),
                moe_gain.reshape(TILES, LANES),
                expert_group,
                inner,
                route_weights.T,
                tokens,
                w_query,
                w_key,
                w_value,
                w_gate,
                state,
                w_out,
                expert_down,
            )
        )
    )

    new_state = pl.pallas_call(
        state_kernel,
        grid=(CHUNKS,),
        out_shape=jax.ShapeDtypeStruct(state.shape, F32),
        in_specs=[
            SMEM,
            pl.BlockSpec((GROUP, HEADS, HD, HD), lambda i: (i, 0, 0, 0)),
            pl.BlockSpec((GROUP, RW), lambda i: (i, 0)),
            pl.BlockSpec((GROUP, RW), lambda i: (i, 0)),
        ],
        out_specs=pl.BlockSpec((GROUP, HEADS, HD, HD), lambda i: (i, 0, 0, 0)),
        cost_estimate=pl.CostEstimate(
            flops=10**9, bytes_accessed=26 * 10**6, transcendentals=0
        ),
        compiler_params=pltpu.CompilerParams(vmem_limit_bytes=20 * 2**20),
        name="state_update",
    )(in_hbm(decay_rate), in_hbm(state), in_vmem(keys), in_vmem(values))

    def dispatch(rows):
        return lax.all_to_all(rows, "ep", split_axis=0, concat_axis=0, tiled=True)

    outputs = pl.pallas_call(
        expert_kernel,
        out_shape=jax.ShapeDtypeStruct(ROW_TILES, BF16),
        in_specs=[VMEM] * 4,
        out_specs=HBM,
        scratch_shapes=[
            pltpu.VMEM((2 * EXPERTS * STEP, LANES), F32),
            pltpu.VMEM((2 * EXPERTS, D), BF16),
            pltpu.VMEM(ROW_TILES, BF16),
            pltpu.SemaphoreType.DMA((COPIES,)),
        ],
        cost_estimate=pl.CostEstimate(
            flops=8 * 10**8, bytes_accessed=4 * 10**6, transcendentals=0
        ),
        compiler_params=pltpu.CompilerParams(vmem_limit_bytes=16 * 2**20),
        name="expert",
    )(
        in_vmem(dispatch(send)),
        in_vmem(expert_gate),
        in_vmem(expert_up),
        in_vmem(down),
    )
    output = pl.pallas_call(
        combine_kernel,
        out_shape=jax.ShapeDtypeStruct((ROWS, D), BF16),
        in_specs=[SMEM, SMEM, VMEM, VMEM],
        out_specs=HBM,
        scratch_shapes=[
            pltpu.VMEM((ROWS * STEP, LANES), F32),
            pltpu.VMEM((ROWS, D), BF16),
            pltpu.SemaphoreType.DMA((ROWS // PART,)),
        ],
        compiler_params=pltpu.CompilerParams(vmem_limit_bytes=8 * 2**20),
        name="combine",
    )(in_smem(slots), in_smem(weights), in_vmem(mixed), in_vmem(dispatch(outputs)))
    return output, new_state


def solution(mesh):
    return jax.shard_map(
        local,
        mesh=mesh,
        in_specs=(
            P("ep", None),
            P("ep"),
            P(),
            P(),
            P(),
            P(),
            P(),
            P(),
            P("ep", None, None, None),
            P(),
            P(),
            P(),
            P("ep", None),
            P("ep"),
            P("ep", None),
            P("ep", None, None),
            P("ep", None, None),
            P("ep", None, None),
        ),
        out_specs=(P("ep", None), P("ep", None, None, None)),
        check_vma=False,
    )
```

```python
import functools

import jax
import jax.numpy as jnp
import numpy as np
from jax import lax
from jax.experimental import pallas as pl
from jax.experimental.pallas import tpu as pltpu
from jax.sharding import PartitionSpec as P

EPS = 1e-06
ROWS = 48
D = 2048
HEADS = 8
HD = 64
RW = HEADS * HD
EXPERTS = 128
LANES = 128
TILES = D // LANES
GROUP = 8
CHUNKS = ROWS // GROUP
STEP = 20
PART = 16
COPIES = 4
F32 = jnp.float32
BF16 = jnp.bfloat16


ORDER = [
    (p % 4) * 32 + (p // 4 % 4) * 8 + (p // 16 % 4) * 2 + p // 64 for p in range(128)
]


def place_of(group, inner):
    return group + (inner // 8) * 4 + (inner // 2 % 4) * 16 + (inner % 2) * 64


def lane_iota(shape):
    return lax.broadcasted_iota(jnp.int32, shape, len(shape) - 1)


def row_iota(shape):
    return lax.broadcasted_iota(jnp.int32, shape, 0)


def split(x):
    high = x.astype(BF16).astype(F32)
    return high, x - high


def by_lanes(f, x):
    return jnp.concatenate(
        [f(x[:, c * LANES : (c + 1) * LANES]) for c in range(x.shape[1] // LANES)],
        axis=1,
    )


def head_sum(x):
    shape = (LANES, LANES)
    ones = (row_iota(shape) // HD == lane_iota(shape) // HD).astype(BF16)

    def part(y):
        high, low = split(y)
        return jnp.dot(high.astype(BF16), ones, preferred_element_type=F32) + jnp.dot(
            low.astype(BF16), ones, preferred_element_type=F32
        )

    return by_lanes(part, x)


def rope(x, cosine, sine):
    first = (lane_iota((ROWS, LANES)) % HD) < (HD // 2)

    def part(y):
        other = jnp.where(
            first, pltpu.roll(y, LANES - HD // 2, 1), pltpu.roll(y, HD // 2, 1)
        )
        return y * cosine + other * sine

    return by_lanes(part, x)


def front_kernel(
    hist_hbm,
    inv_hbm,
    ngain_hbm,
    decay_hbm,
    hgain_hbm,
    mgain_hbm,
    group_hbm,
    inner_hbm,
    weight_hbm,
    tok_hbm,
    wq_hbm,
    wk_hbm,
    wv_hbm,
    wg_hbm,
    state_hbm,
    wo_hbm,
    down_hbm,
    mixed_ref,
    send_ref,
    k_ref,
    v_ref,
    slot_ref,
    weight_ref,
    down_ref,
    hist,
    inv,
    ngain,
    decay,
    hgain,
    mgain,
    group,
    inner,
    seen,
    tok,
    w4,
    wo,
    st,
    qs,
    part,
    wide,
    scales,
    small_sem,
    w_sem,
    st_sem,
):
    small = [
        pltpu.make_async_copy(src, dst, small_sem.at[i])
        for i, (src, dst) in enumerate(
            (
                (tok_hbm, tok),
                (ngain_hbm, ngain),
                (hist_hbm, hist),
                (inv_hbm, inv),
                (decay_hbm, decay),
                (hgain_hbm, hgain),
                (mgain_hbm, mgain),
                (group_hbm, group),
                (inner_hbm, inner),
                (weight_hbm, weight_ref),
            )
        )
    ]
    weights = [
        pltpu.make_async_copy(src, w4.at[i], w_sem.at[i])
        for i, src in enumerate((wq_hbm, wk_hbm, wv_hbm, wg_hbm))
    ]
    wo_copy = pltpu.make_async_copy(wo_hbm, wo, w_sem.at[4])
    down_copy = pltpu.make_async_copy(down_hbm, down_ref, w_sem.at[5])

    def state_copy(i):
        rows = pl.ds(i * GROUP, GROUP)
        return pltpu.make_async_copy(state_hbm.at[rows], st.at[rows], st_sem.at[i])

    for copy in small:
        copy.start()
    for copy in weights:
        copy.start()
    for copy in small:
        copy.wait()
    state_copy(0).start()

    x = tok[...].astype(F32)
    scale = lax.rsqrt(jnp.mean(x * x, axis=-1, keepdims=True) + EPS)
    normed = (x * scale * ngain[...]).astype(BF16)

    square = (ROWS, ROWS)
    place = jnp.sum(
        jnp.where(
            row_iota(square) == lane_iota(square),
            jnp.broadcast_to(hist[...].astype(F32), square),
            0.0,
        ),
        axis=1,
        keepdims=True,
    )
    angles = place * inv[...]
    cosine = jnp.cos(angles)
    sine = jnp.sin(angles)
    sine = jnp.where((lane_iota((ROWS, LANES)) % HD) < (HD // 2), -sine, sine)

    for e in range(EXPERTS):
        seen[e] = 0
    for t in range(ROWS):
        for j in range(2):
            e = place_of(group[t], inner[j, t])
            slot = seen[e]
            seen[e] = 1
            slot_ref[j, t] = 2 * e + slot
    zero = jnp.zeros((TILES, LANES), BF16)
    for e in range(2 * EXPERTS):
        send_ref[e] = zero

    def project(i):
        weights[i].wait()
        return jnp.dot(normed, w4[i], preferred_element_type=F32).astype(BF16).astype(F32)

    q = project(0)
    for i in range(1, 3):
        state_copy(i).start()
    q = rope(q, cosine, sine)
    k = project(1)
    for i in range(3, CHUNKS):
        state_copy(i).start()
    wo_copy.start()
    k = rope(k, cosine, sine) * (HD**-0.5)
    v = project(2)
    down_copy.start()
    gate = project(3)
    for i, piece in enumerate(split(q)):
        qs[i] = piece
    k_ref[...] = k
    v_ref[...] = v

    fresh = head_sum(q * k) * v
    heads = lane_iota((1, RW)) // HD
    rate = jnp.zeros((1, RW), F32)
    for h in range(HEADS):
        rate = jnp.where(heads == h, decay[h], rate)
    retain = jnp.exp(-rate)
    own = row_iota((HEADS, RW)) == lane_iota((HEADS, RW)) // HD

    def read(t):
        spread = [
            jnp.where(own, jnp.broadcast_to(qs[s, pl.ds(t, 1), :], (HEADS, RW)), 0.0)
            for s in range(2)
        ]
        total = jnp.dot(
            jnp.concatenate(spread, axis=0).astype(BF16),
            st[t].reshape(RW, HD).astype(BF16),
            preferred_element_type=F32,
        )
        part[pl.ds(t * (HEADS + 1), HEADS), 0:HD] = (
            total[0:HEADS] + total[HEADS:]
        )

    def chunk(i, carry):
        state_copy(i).wait()
        for b in range(GROUP):
            read(i * GROUP + b)
        return carry

    lax.fori_loop(0, CHUNKS, chunk, 0)

    def head_rows(h):
        return part[pl.ds(h, ROWS, stride=HEADS + 1), :]

    low_half = lane_iota((ROWS, LANES)) < HD
    old = jnp.concatenate(
        [
            jnp.where(
                low_half, head_rows(2 * c), pltpu.roll(head_rows(2 * c + 1), HD, 1)
            )
            for c in range(HEADS // 2)
        ],
        axis=1,
    )
    reading = retain * old + fresh
    mean_square = head_sum(reading * reading) * (1.0 / HD)
    reading = reading * lax.rsqrt(mean_square + EPS) * hgain[...]
    mixed_heads = (reading * jax.nn.silu(gate)).astype(BF16)
    wo_copy.wait()
    squares = jnp.zeros((ROWS, LANES), F32)
    for n in range(0, D, 2 * LANES):
        block = slice(n, n + 2 * LANES)
        mixed = tok[:, block].astype(F32) + jnp.dot(
            mixed_heads, wo[:, block], preferred_element_type=F32
        )
        mixed = mixed.astype(BF16).astype(F32)
        for i in range(2):
            piece = mixed[:, i * LANES : (i + 1) * LANES]
            squares = squares + piece * piece
            wide[pl.ds(n // LANES + i, ROWS, stride=STEP), :] = piece
    scale = lax.rsqrt(jnp.sum(squares, axis=-1, keepdims=True) * (1.0 / D) + EPS)
    scales[...] = jnp.broadcast_to(scale, (ROWS, LANES))
    for t in range(ROWS):
        tile = wide[t * STEP : t * STEP + TILES, :]
        mixed_ref[t] = tile.astype(BF16)
        row = (tile * scales[t : t + 1, :] * mgain[...]).astype(BF16)
        for j in range(2):
            send_ref[slot_ref[j, t]] = row
    down_copy.wait()


def state_kernel(decay, state_ref, k_ref, v_ref, new_ref):
    k = k_ref[...]
    high = k.astype(BF16).astype(F32)
    kt = jnp.concatenate([high, k - high], axis=0).T.astype(BF16)
    v = v_ref[...]
    swapped = jnp.concatenate(
        [
            pltpu.roll(v[:, c * LANES : (c + 1) * LANES], HD, 1)
            for c in range(RW // LANES)
        ],
        axis=1,
    )
    retains = [jnp.exp(jnp.full((HD, HD), -decay[h], F32)) for h in range(HEADS)]
    for pair in range(GROUP // 2):
        shape = (2 * GROUP, 2 * LANES)
        pick = (
            lax.broadcasted_iota(jnp.int32, shape, 0) % GROUP
            == lane_iota(shape) // LANES + 2 * pair
        ).astype(BF16)
        columns = jnp.dot(kt, pick, preferred_element_type=F32)
        for i in range(2):
            b = 2 * pair + i
            for h in range(HEADS):
                column = columns[h * HD : (h + 1) * HD, i * LANES : i * LANES + HD]
                c = (h // 2) * LANES
                row = (swapped if h % 2 else v)[b : b + 1, c : c + HD]
                new_ref[b, h] = retains[h] * state_ref[b, h] + column * row


def expert_kernel(in_ref, wg_ref, wu_ref, wd_ref, out_hbm, wide, lhs, out, sem):
    n = 2 * EXPERTS
    for i in range(n):
        wide[i * STEP : i * STEP + TILES, :] = in_ref[i].astype(F32)
    for r in range(TILES):
        lhs[:, r * LANES : (r + 1) * LANES] = wide[pl.ds(r, n, stride=STEP), :].astype(BF16)
    rows = lhs[...]
    gate = jnp.dot(rows, wg_ref[0], preferred_element_type=F32)
    up = jnp.dot(rows, wu_ref[0], preferred_element_type=F32)
    hidden = (jax.nn.silu(gate) * up).astype(BF16)
    result = jnp.dot(hidden, wd_ref[0], preferred_element_type=F32)
    for r in range(TILES):
        wide[pl.ds(r, n, stride=STEP), :] = result[:, r * LANES : (r + 1) * LANES]
    copies = []
    for c in range(COPIES):
        for i in range(c * n // COPIES, (c + 1) * n // COPIES):
            out[i] = wide[i * STEP : i * STEP + TILES, :].astype(BF16)
        rows = pl.ds(c * n // COPIES, n // COPIES)
        copy = pltpu.make_async_copy(out.at[rows], out_hbm.at[rows], sem.at[c])
        copy.start()
        copies.append(copy)
    for copy in copies:
        copy.wait()


def combine_kernel(slot, weight, mixed_ref, back_ref, out_hbm, wide, out, sem):
    copies = []
    for i in range(ROWS // PART):
        for t in range(i * PART, (i + 1) * PART):
            total = mixed_ref[t].astype(F32)
            for j in range(2):
                total = total + back_ref[slot[j, t]].astype(F32) * weight[j, t]
            wide[t * STEP : t * STEP + TILES, :] = total
        rows = pl.ds(i * PART, PART)
        for r in range(TILES):
            out[rows, r * LANES : (r + 1) * LANES] = wide[
                pl.ds(i * PART * STEP + r, PART, stride=STEP), :
            ].astype(BF16)
        copy = pltpu.make_async_copy(out.at[rows], out_hbm.at[rows], sem.at[i])
        copy.start()
        copies.append(copy)
    for copy in copies:
        copy.wait()


def in_vmem(x):
    return pltpu.with_memory_space_constraint(x, pltpu.VMEM)


def in_smem(x):
    return pltpu.with_memory_space_constraint(x, pltpu.SMEM)


def in_hbm(x):
    return pltpu.with_memory_space_constraint(x, pltpu.HBM)


HBM = pl.BlockSpec(memory_space=pltpu.HBM)
VMEM = pl.BlockSpec(memory_space=pltpu.VMEM)
SMEM = pl.BlockSpec(memory_space=pltpu.SMEM)
ROW_TILES = (2 * EXPERTS, TILES, LANES)


def local(
    tokens,
    history_length,
    norm_gain,
    w_query,
    w_key,
    w_value,
    w_gate,
    decay_rate,
    state,
    head_gain,
    w_out,
    moe_gain,
    route_weights,
    expert_group,
    expert_inner,
    expert_gate,
    expert_up,
    expert_down,
):
    inner = expert_inner.T
    inverse = jnp.asarray(
        (10000.0 ** (-(np.arange(LANES) % 32) / 32.0)).astype(np.float32).reshape(1, LANES)
    )
    mixed, send, keys, values, slots, weights, down = pl.pallas_call(
        front_kernel,
        out_shape=[
            pltpu.VMEM((ROWS, TILES, LANES), BF16),
            pltpu.VMEM(ROW_TILES, BF16),
            pltpu.VMEM((ROWS, RW), F32),
            pltpu.VMEM((ROWS, RW), F32),
            pltpu.SMEM((2, ROWS), jnp.int32),
            pltpu.SMEM((2, ROWS), F32),
            pltpu.VMEM(expert_down.shape, BF16),
        ],
        in_specs=[HBM] * 17,
        out_specs=[VMEM, VMEM, VMEM, VMEM, SMEM, SMEM, VMEM],
        scratch_shapes=[
            pltpu.VMEM((1, ROWS), jnp.int32),
            pltpu.VMEM((1, LANES), F32),
            pltpu.VMEM((1, D), F32),
            pltpu.SMEM((HEADS,), F32),
            pltpu.VMEM((1, RW), F32),
            pltpu.VMEM((TILES, LANES), F32),
            pltpu.SMEM((ROWS,), jnp.int32),
            pltpu.SMEM((2, ROWS), jnp.int32),
            pltpu.SMEM((EXPERTS,), jnp.int32),
            pltpu.VMEM((ROWS, D), BF16),
            pltpu.VMEM((4, D, RW), BF16),
            pltpu.VMEM((RW, D), BF16),
            pltpu.VMEM((ROWS, HEADS, HD, HD), F32),
            pltpu.VMEM((2, ROWS, RW), F32),
            pltpu.VMEM(((HEADS + 1) * ROWS, LANES), F32),
            pltpu.VMEM((ROWS * STEP, LANES), F32),
            pltpu.VMEM((ROWS, LANES), F32),
            pltpu.SemaphoreType.DMA((10,)),
            pltpu.SemaphoreType.DMA((6,)),
            pltpu.SemaphoreType.DMA((CHUNKS,)),
        ],
        compiler_params=pltpu.CompilerParams(vmem_limit_bytes=32 * 2**20),
        name="front",
    )(
        *(
            in_hbm(x)
            for x in (
                history_length.reshape(1, ROWS),
                inverse,
                norm_gain.reshape(1, D),
                decay_rate,
                head_gain.reshape(1, RW),
                moe_gain.reshape(TILES, LANES),
                expert_group,
                inner,
                route_weights.T,
                tokens,
                w_query,
                w_key,
                w_value,
                w_gate,
                state,
                w_out,
                expert_down,
            )
        )
    )

    new_state = pl.pallas_call(
        state_kernel,
        grid=(CHUNKS,),
        out_shape=jax.ShapeDtypeStruct(state.shape, F32),
        in_specs=[
            SMEM,
            pl.BlockSpec((GROUP, HEADS, HD, HD), lambda i: (i, 0, 0, 0)),
            pl.BlockSpec((GROUP, RW), lambda i: (i, 0)),
            pl.BlockSpec((GROUP, RW), lambda i: (i, 0)),
        ],
        out_specs=pl.BlockSpec((GROUP, HEADS, HD, HD), lambda i: (i, 0, 0, 0)),
        cost_estimate=pl.CostEstimate(
            flops=10**9, bytes_accessed=26 * 10**6, transcendentals=0
        ),
        compiler_params=pltpu.CompilerParams(vmem_limit_bytes=20 * 2**20),
        name="state_update",
    )(in_hbm(decay_rate), in_hbm(state), in_vmem(keys), in_vmem(values))

    def dispatch(rows):
        return lax.all_to_all(
            rows,
            "ep",
            split_axis=0,
            concat_axis=0,
            axis_index_groups=[ORDER],
            tiled=True,
        )

    outputs = pl.pallas_call(
        expert_kernel,
        out_shape=jax.ShapeDtypeStruct(ROW_TILES, BF16),
        in_specs=[VMEM] * 4,
        out_specs=HBM,
        scratch_shapes=[
            pltpu.VMEM((2 * EXPERTS * STEP, LANES), F32),
            pltpu.VMEM((2 * EXPERTS, D), BF16),
            pltpu.VMEM(ROW_TILES, BF16),
            pltpu.SemaphoreType.DMA((COPIES,)),
        ],
        cost_estimate=pl.CostEstimate(
            flops=8 * 10**8, bytes_accessed=4 * 10**6, transcendentals=0
        ),
        compiler_params=pltpu.CompilerParams(vmem_limit_bytes=16 * 2**20),
        name="expert",
    )(
        in_vmem(dispatch(send)),
        in_vmem(expert_gate),
        in_vmem(expert_up),
        in_vmem(down),
    )
    output = pl.pallas_call(
        combine_kernel,
        out_shape=jax.ShapeDtypeStruct((ROWS, D), BF16),
        in_specs=[SMEM, SMEM, VMEM, VMEM],
        out_specs=HBM,
        scratch_shapes=[
            pltpu.VMEM((ROWS * STEP, LANES), F32),
            pltpu.VMEM((ROWS, D), BF16),
            pltpu.SemaphoreType.DMA((ROWS // PART,)),
        ],
        compiler_params=pltpu.CompilerParams(vmem_limit_bytes=8 * 2**20),
        name="combine",
    )(in_smem(slots), in_smem(weights), in_vmem(mixed), in_vmem(dispatch(outputs)))
    return output, new_state


def solution(mesh):
    return jax.shard_map(
        local,
        mesh=mesh,
        in_specs=(
            P("ep", None),
            P("ep"),
            P(),
            P(),
            P(),
            P(),
            P(),
            P(),
            P("ep", None, None, None),
            P(),
            P(),
            P(),
            P("ep", None),
            P("ep"),
            P("ep", None),
            P("ep", None, None),
            P("ep", None, None),
            P("ep", None, None),
        ),
        out_specs=(P("ep", None), P("ep", None, None, None)),
        check_vma=False,
    )
```

```python
import functools

import jax
import jax.numpy as jnp
import numpy as np
from jax import lax
from jax.experimental import pallas as pl
from jax.experimental.pallas import tpu as pltpu
from jax.sharding import PartitionSpec as P

EPS = 1e-06
ROWS = 48
D = 2048
HEADS = 8
HD = 64
RW = HEADS * HD
EXPERTS = 128
LANES = 128
TILES = D // LANES
GROUP = 8
CHUNKS = ROWS // GROUP
STEP = 20
PART = 16
COPIES = 4
F32 = jnp.float32
BF16 = jnp.bfloat16


SHIFT = 21
OUT_ORDER = [
    ((p % 4) * 32 + (p // 4 % 4) * 8 + (p // 16 % 4) * 2 + p // 64) ^ SHIFT
    for p in range(128)
]
BACK_ORDER = [
    (p % 4) * 32 + (p // 16 % 4) * 8 + (p // 4 % 4) * 2 + p // 64 for p in range(128)
]


def out_place(group, inner):
    inner = inner ^ SHIFT
    return group + (inner // 8) * 4 + (inner // 2 % 4) * 16 + (inner % 2) * 64


def back_place(group, inner):
    return group + (inner // 2 % 4) * 4 + (inner // 8) * 16 + (inner % 2) * 64


def lane_iota(shape):
    return lax.broadcasted_iota(jnp.int32, shape, len(shape) - 1)


def row_iota(shape):
    return lax.broadcasted_iota(jnp.int32, shape, 0)


def split(x):
    high = x.astype(BF16).astype(F32)
    return high, x - high


def by_lanes(f, x):
    return jnp.concatenate(
        [f(x[:, c * LANES : (c + 1) * LANES]) for c in range(x.shape[1] // LANES)],
        axis=1,
    )


def head_sum(x):
    shape = (LANES, LANES)
    ones = (row_iota(shape) // HD == lane_iota(shape) // HD).astype(BF16)

    def part(y):
        high, low = split(y)
        return jnp.dot(high.astype(BF16), ones, preferred_element_type=F32) + jnp.dot(
            low.astype(BF16), ones, preferred_element_type=F32
        )

    return by_lanes(part, x)


def rope(x, cosine, sine):
    first = (lane_iota((ROWS, LANES)) % HD) < (HD // 2)

    def part(y):
        other = jnp.where(
            first, pltpu.roll(y, LANES - HD // 2, 1), pltpu.roll(y, HD // 2, 1)
        )
        return y * cosine + other * sine

    return by_lanes(part, x)


def front_kernel(
    hist_hbm,
    inv_hbm,
    ngain_hbm,
    decay_hbm,
    hgain_hbm,
    mgain_hbm,
    group_hbm,
    inner_hbm,
    weight_hbm,
    tok_hbm,
    wq_hbm,
    wk_hbm,
    wv_hbm,
    wg_hbm,
    state_hbm,
    wo_hbm,
    down_hbm,
    mixed_ref,
    send_ref,
    k_ref,
    v_ref,
    slot_ref,
    weight_ref,
    down_ref,
    hist,
    inv,
    ngain,
    decay,
    hgain,
    mgain,
    group,
    inner,
    seen,
    target,
    tok,
    w4,
    wo,
    st,
    qs,
    part,
    wide,
    scales,
    small_sem,
    w_sem,
    st_sem,
):
    small = [
        pltpu.make_async_copy(src, dst, small_sem.at[i])
        for i, (src, dst) in enumerate(
            (
                (tok_hbm, tok),
                (ngain_hbm, ngain),
                (hist_hbm, hist),
                (inv_hbm, inv),
                (decay_hbm, decay),
                (hgain_hbm, hgain),
                (mgain_hbm, mgain),
                (group_hbm, group),
                (inner_hbm, inner),
                (weight_hbm, weight_ref),
            )
        )
    ]
    weights = [
        pltpu.make_async_copy(src, w4.at[i], w_sem.at[i])
        for i, src in enumerate((wq_hbm, wk_hbm, wv_hbm, wg_hbm))
    ]
    wo_copy = pltpu.make_async_copy(wo_hbm, wo, w_sem.at[4])
    down_copy = pltpu.make_async_copy(down_hbm, down_ref, w_sem.at[5])

    def state_copy(i):
        rows = pl.ds(i * GROUP, GROUP)
        return pltpu.make_async_copy(state_hbm.at[rows], st.at[rows], st_sem.at[i])

    for copy in small:
        copy.start()
    for copy in weights:
        copy.start()
    for copy in small:
        copy.wait()
    state_copy(0).start()

    x = tok[...].astype(F32)
    scale = lax.rsqrt(jnp.mean(x * x, axis=-1, keepdims=True) + EPS)
    normed = (x * scale * ngain[...]).astype(BF16)

    square = (ROWS, ROWS)
    place = jnp.sum(
        jnp.where(
            row_iota(square) == lane_iota(square),
            jnp.broadcast_to(hist[...].astype(F32), square),
            0.0,
        ),
        axis=1,
        keepdims=True,
    )
    angles = place * inv[...]
    cosine = jnp.cos(angles)
    sine = jnp.sin(angles)
    sine = jnp.where((lane_iota((ROWS, LANES)) % HD) < (HD // 2), -sine, sine)

    for e in range(EXPERTS):
        seen[e] = 0
    for t in range(ROWS):
        for j in range(2):
            e = out_place(group[t], inner[j, t])
            slot = seen[e]
            seen[e] = 1
            target[j, t] = 2 * e + slot
            slot_ref[j, t] = 2 * back_place(group[t], inner[j, t]) + slot
    zero = jnp.zeros((TILES, LANES), BF16)
    for e in range(2 * EXPERTS):
        send_ref[e] = zero

    def project(i):
        weights[i].wait()
        return jnp.dot(normed, w4[i], preferred_element_type=F32).astype(BF16).astype(F32)

    q = project(0)
    for i in range(1, 3):
        state_copy(i).start()
    q = rope(q, cosine, sine)
    k = project(1)
    for i in range(3, CHUNKS):
        state_copy(i).start()
    wo_copy.start()
    k = rope(k, cosine, sine) * (HD**-0.5)
    v = project(2)
    down_copy.start()
    gate = project(3)
    for i, piece in enumerate(split(q)):
        qs[i] = piece
    k_ref[...] = k
    v_ref[...] = v

    fresh = head_sum(q * k) * v
    heads = lane_iota((1, RW)) // HD
    rate = jnp.zeros((1, RW), F32)
    for h in range(HEADS):
        rate = jnp.where(heads == h, decay[h], rate)
    retain = jnp.exp(-rate)
    own = row_iota((HEADS, RW)) == lane_iota((HEADS, RW)) // HD

    def read(t):
        spread = [
            jnp.where(own, jnp.broadcast_to(qs[s, pl.ds(t, 1), :], (HEADS, RW)), 0.0)
            for s in range(2)
        ]
        total = jnp.dot(
            jnp.concatenate(spread, axis=0).astype(BF16),
            st[t].reshape(RW, HD).astype(BF16),
            preferred_element_type=F32,
        )
        part[pl.ds(t * (HEADS + 1), HEADS), 0:HD] = (
            total[0:HEADS] + total[HEADS:]
        )

    def chunk(i, carry):
        state_copy(i).wait()
        for b in range(GROUP):
            read(i * GROUP + b)
        return carry

    lax.fori_loop(0, CHUNKS, chunk, 0)

    def head_rows(h):
        return part[pl.ds(h, ROWS, stride=HEADS + 1), :]

    low_half = lane_iota((ROWS, LANES)) < HD
    old = jnp.concatenate(
        [
            jnp.where(
                low_half, head_rows(2 * c), pltpu.roll(head_rows(2 * c + 1), HD, 1)
            )
            for c in range(HEADS // 2)
        ],
        axis=1,
    )
    reading = retain * old + fresh
    mean_square = head_sum(reading * reading) * (1.0 / HD)
    reading = reading * lax.rsqrt(mean_square + EPS) * hgain[...]
    mixed_heads = (reading * jax.nn.silu(gate)).astype(BF16)
    wo_copy.wait()
    squares = jnp.zeros((ROWS, LANES), F32)
    for n in range(0, D, 2 * LANES):
        block = slice(n, n + 2 * LANES)
        mixed = tok[:, block].astype(F32) + jnp.dot(
            mixed_heads, wo[:, block], preferred_element_type=F32
        )
        mixed = mixed.astype(BF16).astype(F32)
        for i in range(2):
            piece = mixed[:, i * LANES : (i + 1) * LANES]
            squares = squares + piece * piece
            wide[pl.ds(n // LANES + i, ROWS, stride=STEP), :] = piece
    scale = lax.rsqrt(jnp.sum(squares, axis=-1, keepdims=True) * (1.0 / D) + EPS)
    scales[...] = jnp.broadcast_to(scale, (ROWS, LANES))
    for t in range(ROWS):
        tile = wide[t * STEP : t * STEP + TILES, :]
        mixed_ref[t] = tile.astype(BF16)
        row = (tile * scales[t : t + 1, :] * mgain[...]).astype(BF16)
        for j in range(2):
            send_ref[target[j, t]] = row
    down_copy.wait()


def state_kernel(decay, state_ref, k_ref, v_ref, new_ref):
    k = k_ref[...]
    high = k.astype(BF16).astype(F32)
    kt = jnp.concatenate([high, k - high], axis=0).T.astype(BF16)
    v = v_ref[...]
    swapped = jnp.concatenate(
        [
            pltpu.roll(v[:, c * LANES : (c + 1) * LANES], HD, 1)
            for c in range(RW // LANES)
        ],
        axis=1,
    )
    retains = [jnp.exp(jnp.full((HD, HD), -decay[h], F32)) for h in range(HEADS)]
    for pair in range(GROUP // 2):
        shape = (2 * GROUP, 2 * LANES)
        pick = (
            lax.broadcasted_iota(jnp.int32, shape, 0) % GROUP
            == lane_iota(shape) // LANES + 2 * pair
        ).astype(BF16)
        columns = jnp.dot(kt, pick, preferred_element_type=F32)
        for i in range(2):
            b = 2 * pair + i
            for h in range(HEADS):
                column = columns[h * HD : (h + 1) * HD, i * LANES : i * LANES + HD]
                c = (h // 2) * LANES
                row = (swapped if h % 2 else v)[b : b + 1, c : c + HD]
                new_ref[b, h] = retains[h] * state_ref[b, h] + column * row


def expert_kernel(in_ref, wg_ref, wu_ref, wd_ref, out_hbm, wide, lhs, out, sem):
    n = 2 * EXPERTS
    for i in range(n):
        wide[i * STEP : i * STEP + TILES, :] = in_ref[i].astype(F32)
    for r in range(TILES):
        lhs[:, r * LANES : (r + 1) * LANES] = wide[pl.ds(r, n, stride=STEP), :].astype(BF16)
    rows = lhs[...]
    gate = jnp.dot(rows, wg_ref[0], preferred_element_type=F32)
    up = jnp.dot(rows, wu_ref[0], preferred_element_type=F32)
    hidden = (jax.nn.silu(gate) * up).astype(BF16)
    result = jnp.dot(hidden, wd_ref[0], preferred_element_type=F32)
    for r in range(TILES):
        wide[pl.ds(r, n, stride=STEP), :] = result[:, r * LANES : (r + 1) * LANES]
    copies = []
    for c in range(COPIES):
        for i in range(c * n // COPIES, (c + 1) * n // COPIES):
            k = 2 * OUT_ORDER.index(BACK_ORDER[i // 2]) + i % 2
            out[i] = wide[k * STEP : k * STEP + TILES, :].astype(BF16)
        rows = pl.ds(c * n // COPIES, n // COPIES)
        copy = pltpu.make_async_copy(out.at[rows], out_hbm.at[rows], sem.at[c])
        copy.start()
        copies.append(copy)
    for copy in copies:
        copy.wait()


def combine_kernel(slot, weight, mixed_ref, back_ref, out_hbm, wide, out, sem):
    copies = []
    for i in range(ROWS // PART):
        for t in range(i * PART, (i + 1) * PART):
            total = mixed_ref[t].astype(F32)
            for j in range(2):
                total = total + back_ref[slot[j, t]].astype(F32) * weight[j, t]
            wide[t * STEP : t * STEP + TILES, :] = total
        rows = pl.ds(i * PART, PART)
        for r in range(TILES):
            out[rows, r * LANES : (r + 1) * LANES] = wide[
                pl.ds(i * PART * STEP + r, PART, stride=STEP), :
            ].astype(BF16)
        copy = pltpu.make_async_copy(out.at[rows], out_hbm.at[rows], sem.at[i])
        copy.start()
        copies.append(copy)
    for copy in copies:
        copy.wait()


def in_vmem(x):
    return pltpu.with_memory_space_constraint(x, pltpu.VMEM)


def in_smem(x):
    return pltpu.with_memory_space_constraint(x, pltpu.SMEM)


def in_hbm(x):
    return pltpu.with_memory_space_constraint(x, pltpu.HBM)


HBM = pl.BlockSpec(memory_space=pltpu.HBM)
VMEM = pl.BlockSpec(memory_space=pltpu.VMEM)
SMEM = pl.BlockSpec(memory_space=pltpu.SMEM)
ROW_TILES = (2 * EXPERTS, TILES, LANES)


def local(
    tokens,
    history_length,
    norm_gain,
    w_query,
    w_key,
    w_value,
    w_gate,
    decay_rate,
    state,
    head_gain,
    w_out,
    moe_gain,
    route_weights,
    expert_group,
    expert_inner,
    expert_gate,
    expert_up,
    expert_down,
):
    inner = expert_inner.T
    inverse = jnp.asarray(
        (10000.0 ** (-(np.arange(LANES) % 32) / 32.0)).astype(np.float32).reshape(1, LANES)
    )
    mixed, send, keys, values, slots, weights, down = pl.pallas_call(
        front_kernel,
        out_shape=[
            pltpu.VMEM((ROWS, TILES, LANES), BF16),
            pltpu.VMEM(ROW_TILES, BF16),
            pltpu.VMEM((ROWS, RW), F32),
            pltpu.VMEM((ROWS, RW), F32),
            pltpu.SMEM((2, ROWS), jnp.int32),
            pltpu.SMEM((2, ROWS), F32),
            pltpu.VMEM(expert_down.shape, BF16),
        ],
        in_specs=[HBM] * 17,
        out_specs=[VMEM, VMEM, VMEM, VMEM, SMEM, SMEM, VMEM],
        scratch_shapes=[
            pltpu.VMEM((1, ROWS), jnp.int32),
            pltpu.VMEM((1, LANES), F32),
            pltpu.VMEM((1, D), F32),
            pltpu.SMEM((HEADS,), F32),
            pltpu.VMEM((1, RW), F32),
            pltpu.VMEM((TILES, LANES), F32),
            pltpu.SMEM((ROWS,), jnp.int32),
            pltpu.SMEM((2, ROWS), jnp.int32),
            pltpu.SMEM((EXPERTS,), jnp.int32),
            pltpu.SMEM((2, ROWS), jnp.int32),
            pltpu.VMEM((ROWS, D), BF16),
            pltpu.VMEM((4, D, RW), BF16),
            pltpu.VMEM((RW, D), BF16),
            pltpu.VMEM((ROWS, HEADS, HD, HD), F32),
            pltpu.VMEM((2, ROWS, RW), F32),
            pltpu.VMEM(((HEADS + 1) * ROWS, LANES), F32),
            pltpu.VMEM((ROWS * STEP, LANES), F32),
            pltpu.VMEM((ROWS, LANES), F32),
            pltpu.SemaphoreType.DMA((10,)),
            pltpu.SemaphoreType.DMA((6,)),
            pltpu.SemaphoreType.DMA((CHUNKS,)),
        ],
        compiler_params=pltpu.CompilerParams(vmem_limit_bytes=32 * 2**20),
        name="front",
    )(
        *(
            in_hbm(x)
            for x in (
                history_length.reshape(1, ROWS),
                inverse,
                norm_gain.reshape(1, D),
                decay_rate,
                head_gain.reshape(1, RW),
                moe_gain.reshape(TILES, LANES),
                expert_group,
                inner,
                route_weights.T,
                tokens,
                w_query,
                w_key,
                w_value,
                w_gate,
                state,
                w_out,
                expert_down,
            )
        )
    )

    new_state = pl.pallas_call(
        state_kernel,
        grid=(CHUNKS,),
        out_shape=jax.ShapeDtypeStruct(state.shape, F32),
        in_specs=[
            SMEM,
            pl.BlockSpec((GROUP, HEADS, HD, HD), lambda i: (i, 0, 0, 0)),
            pl.BlockSpec((GROUP, RW), lambda i: (i, 0)),
            pl.BlockSpec((GROUP, RW), lambda i: (i, 0)),
        ],
        out_specs=pl.BlockSpec((GROUP, HEADS, HD, HD), lambda i: (i, 0, 0, 0)),
        cost_estimate=pl.CostEstimate(
            flops=10**9, bytes_accessed=26 * 10**6, transcendentals=0
        ),
        compiler_params=pltpu.CompilerParams(vmem_limit_bytes=20 * 2**20),
        name="state_update",
    )(in_hbm(decay_rate), in_hbm(state), in_vmem(keys), in_vmem(values))

    def exchange(rows, order):
        return lax.all_to_all(
            rows,
            "ep",
            split_axis=0,
            concat_axis=0,
            axis_index_groups=[order],
            tiled=True,
        )

    outputs = pl.pallas_call(
        expert_kernel,
        out_shape=jax.ShapeDtypeStruct(ROW_TILES, BF16),
        in_specs=[VMEM] * 4,
        out_specs=HBM,
        scratch_shapes=[
            pltpu.VMEM((2 * EXPERTS * STEP, LANES), F32),
            pltpu.VMEM((2 * EXPERTS, D), BF16),
            pltpu.VMEM(ROW_TILES, BF16),
            pltpu.SemaphoreType.DMA((COPIES,)),
        ],
        cost_estimate=pl.CostEstimate(
            flops=8 * 10**8, bytes_accessed=4 * 10**6, transcendentals=0
        ),
        compiler_params=pltpu.CompilerParams(vmem_limit_bytes=16 * 2**20),
        name="expert",
    )(
        in_vmem(exchange(send, OUT_ORDER)),
        in_vmem(expert_gate),
        in_vmem(expert_up),
        in_vmem(down),
    )
    output = pl.pallas_call(
        combine_kernel,
        out_shape=jax.ShapeDtypeStruct((ROWS, D), BF16),
        in_specs=[SMEM, SMEM, VMEM, VMEM],
        out_specs=HBM,
        scratch_shapes=[
            pltpu.VMEM((ROWS * STEP, LANES), F32),
            pltpu.VMEM((ROWS, D), BF16),
            pltpu.SemaphoreType.DMA((ROWS // PART,)),
        ],
        compiler_params=pltpu.CompilerParams(vmem_limit_bytes=8 * 2**20),
        name="combine",
    )(in_smem(slots), in_smem(weights), in_vmem(mixed), in_vmem(exchange(outputs, BACK_ORDER)))
    return output, new_state


def solution(mesh):
    return jax.shard_map(
        local,
        mesh=mesh,
        in_specs=(
            P("ep", None),
            P("ep"),
            P(),
            P(),
            P(),
            P(),
            P(),
            P(),
            P("ep", None, None, None),
            P(),
            P(),
            P(),
            P("ep", None),
            P("ep"),
            P("ep", None),
            P("ep", None, None),
            P("ep", None, None),
            P("ep", None, None),
        ),
        out_specs=(P("ep", None), P("ep", None, None, None)),
        check_vma=False,
    )
```

```python
import functools

import jax
import jax.numpy as jnp
import numpy as np
from jax import lax
from jax.experimental import pallas as pl
from jax.experimental.pallas import tpu as pltpu
from jax.sharding import PartitionSpec as P

EPS = 1e-06
ROWS = 48
D = 2048
HEADS = 8
HD = 64
RW = HEADS * HD
EXPERTS = 128
LANES = 128
TILES = D // LANES
GROUP = 8
CHUNKS = ROWS // GROUP
STEP = 20
PART = 16
COPIES = 4
F32 = jnp.float32
BF16 = jnp.bfloat16


SHIFT = 21
OUT_ORDER = [
    ((p % 4) * 32 + (p // 4 % 4) * 8 + (p // 16 % 4) * 2 + p // 64) ^ SHIFT
    for p in range(128)
]
BACK_ORDER = [
    (p % 4) * 32 + (p // 16 % 4) * 8 + (p // 4 % 4) * 2 + p // 64 for p in range(128)
]


def out_place(group, inner):
    inner = inner ^ SHIFT
    return group + (inner >> 3) * 4 + (inner >> 1 & 3) * 16 + (inner & 1) * 64


def back_place(group, inner):
    return group + (inner >> 1 & 3) * 4 + (inner >> 3) * 16 + (inner & 1) * 64


def lane_iota(shape):
    return lax.broadcasted_iota(jnp.int32, shape, len(shape) - 1)


def row_iota(shape):
    return lax.broadcasted_iota(jnp.int32, shape, 0)


def split(x):
    high = x.astype(BF16).astype(F32)
    return high, x - high


def by_lanes(f, x):
    return jnp.concatenate(
        [f(x[:, c * LANES : (c + 1) * LANES]) for c in range(x.shape[1] // LANES)],
        axis=1,
    )


def head_sum(x):
    shape = (LANES, LANES)
    ones = (row_iota(shape) // HD == lane_iota(shape) // HD).astype(BF16)

    def part(y):
        high, low = split(y)
        return jnp.dot(high.astype(BF16), ones, preferred_element_type=F32) + jnp.dot(
            low.astype(BF16), ones, preferred_element_type=F32
        )

    return by_lanes(part, x)


def rope(x, cosine, sine):
    first = (lane_iota((ROWS, LANES)) % HD) < (HD // 2)

    def part(y):
        other = jnp.where(
            first, pltpu.roll(y, LANES - HD // 2, 1), pltpu.roll(y, HD // 2, 1)
        )
        return y * cosine + other * sine

    return by_lanes(part, x)


def front_kernel(
    hist_hbm,
    inv_hbm,
    ngain_hbm,
    decay_hbm,
    hgain_hbm,
    mgain_hbm,
    group_hbm,
    inner_hbm,
    weight_hbm,
    tok_hbm,
    wq_hbm,
    wk_hbm,
    wv_hbm,
    wg_hbm,
    state_hbm,
    wo_hbm,
    down_hbm,
    mixed_ref,
    send_ref,
    k_ref,
    v_ref,
    slot_ref,
    weight_ref,
    down_ref,
    hist,
    inv,
    ngain,
    decay,
    hgain,
    mgain,
    group,
    inner,
    seen,
    target,
    tok,
    w4,
    wo,
    st,
    qs,
    part,
    wide,
    scales,
    small_sem,
    w_sem,
    st_sem,
):
    small = [
        pltpu.make_async_copy(src, dst, small_sem.at[i])
        for i, (src, dst) in enumerate(
            (
                (tok_hbm, tok),
                (ngain_hbm, ngain),
                (hist_hbm, hist),
                (inv_hbm, inv),
                (decay_hbm, decay),
                (hgain_hbm, hgain),
                (mgain_hbm, mgain),
                (group_hbm, group),
                (inner_hbm, inner),
                (weight_hbm, weight_ref),
            )
        )
    ]
    weights = [
        pltpu.make_async_copy(src, w4.at[i], w_sem.at[i])
        for i, src in enumerate((wq_hbm, wk_hbm, wv_hbm, wg_hbm))
    ]
    wo_copy = pltpu.make_async_copy(wo_hbm, wo, w_sem.at[4])
    down_copy = pltpu.make_async_copy(down_hbm, down_ref, w_sem.at[5])

    def state_copy(i):
        rows = pl.ds(i * GROUP, GROUP)
        return pltpu.make_async_copy(state_hbm.at[rows], st.at[rows], st_sem.at[i])

    for copy in small:
        copy.start()
    for copy in weights:
        copy.start()
    for copy in small:
        copy.wait()
    state_copy(0).start()

    x = tok[...].astype(F32)
    scale = lax.rsqrt(jnp.mean(x * x, axis=-1, keepdims=True) + EPS)
    normed = (x * scale * ngain[...]).astype(BF16)

    square = (ROWS, ROWS)
    place = jnp.sum(
        jnp.where(
            row_iota(square) == lane_iota(square),
            jnp.broadcast_to(hist[...].astype(F32), square),
            0.0,
        ),
        axis=1,
        keepdims=True,
    )
    angles = place * inv[...]
    cosine = jnp.cos(angles)
    sine = jnp.sin(angles)
    sine = jnp.where((lane_iota((ROWS, LANES)) % HD) < (HD // 2), -sine, sine)

    for e in range(EXPERTS):
        seen[e] = 0
    for t in range(ROWS):
        for j in range(2):
            e = out_place(group[t], inner[j, t])
            slot = seen[e]
            seen[e] = 1
            target[j, t] = 2 * e + slot
            slot_ref[j, t] = 2 * back_place(group[t], inner[j, t]) + slot
    zero = jnp.zeros((TILES, LANES), BF16)
    for e in range(2 * EXPERTS):
        send_ref[e] = zero

    def project(i):
        weights[i].wait()
        return jnp.dot(normed, w4[i], preferred_element_type=F32).astype(BF16).astype(F32)

    q = project(0)
    for i in range(1, 3):
        state_copy(i).start()
    q = rope(q, cosine, sine)
    k = project(1)
    for i in range(3, CHUNKS):
        state_copy(i).start()
    wo_copy.start()
    k = rope(k, cosine, sine) * (HD**-0.5)
    v = project(2)
    down_copy.start()
    gate = project(3)
    for i, piece in enumerate(split(q)):
        qs[i] = piece
    k_ref[...] = k
    v_ref[...] = v

    fresh = head_sum(q * k) * v
    heads = lane_iota((1, RW)) // HD
    rate = jnp.zeros((1, RW), F32)
    for h in range(HEADS):
        rate = jnp.where(heads == h, decay[h], rate)
    retain = jnp.exp(-rate)
    own = row_iota((HEADS, RW)) == lane_iota((HEADS, RW)) // HD

    def read(t):
        spread = [
            jnp.where(own, jnp.broadcast_to(qs[s, pl.ds(t, 1), :], (HEADS, RW)), 0.0)
            for s in range(2)
        ]
        total = jnp.dot(
            jnp.concatenate(spread, axis=0).astype(BF16),
            st[t].reshape(RW, HD).astype(BF16),
            preferred_element_type=F32,
        )
        part[pl.ds(t * (HEADS + 1), HEADS), 0:HD] = (
            total[0:HEADS] + total[HEADS:]
        )

    def chunk(i, carry):
        state_copy(i).wait()
        for b in range(GROUP):
            read(i * GROUP + b)
        return carry

    lax.fori_loop(0, CHUNKS, chunk, 0)

    def head_rows(h):
        return part[pl.ds(h, ROWS, stride=HEADS + 1), :]

    low_half = lane_iota((ROWS, LANES)) < HD
    old = jnp.concatenate(
        [
            jnp.where(
                low_half, head_rows(2 * c), pltpu.roll(head_rows(2 * c + 1), HD, 1)
            )
            for c in range(HEADS // 2)
        ],
        axis=1,
    )
    reading = retain * old + fresh
    mean_square = head_sum(reading * reading) * (1.0 / HD)
    reading = reading * lax.rsqrt(mean_square + EPS) * hgain[...]
    mixed_heads = (reading * jax.nn.silu(gate)).astype(BF16)
    wo_copy.wait()
    squares = jnp.zeros((ROWS, LANES), F32)
    for n in range(0, D, 2 * LANES):
        block = slice(n, n + 2 * LANES)
        mixed = tok[:, block].astype(F32) + jnp.dot(
            mixed_heads, wo[:, block], preferred_element_type=F32
        )
        mixed = mixed.astype(BF16).astype(F32)
        for i in range(2):
            piece = mixed[:, i * LANES : (i + 1) * LANES]
            squares = squares + piece * piece
            wide[pl.ds(n // LANES + i, ROWS, stride=STEP), :] = piece
    scale = lax.rsqrt(jnp.sum(squares, axis=-1, keepdims=True) * (1.0 / D) + EPS)
    scales[...] = jnp.broadcast_to(scale, (ROWS, LANES))
    for t in range(ROWS):
        tile = wide[t * STEP : t * STEP + TILES, :]
        mixed_ref[t] = tile.astype(BF16)
        row = (tile * scales[t : t + 1, :] * mgain[...]).astype(BF16)
        for j in range(2):
            send_ref[target[j, t]] = row
    down_copy.wait()


def state_kernel(decay, state_ref, k_ref, v_ref, new_ref):
    k = k_ref[...]
    high = k.astype(BF16).astype(F32)
    kt = jnp.concatenate([high, k - high], axis=0).T.astype(BF16)
    v = v_ref[...]
    swapped = jnp.concatenate(
        [
            pltpu.roll(v[:, c * LANES : (c + 1) * LANES], HD, 1)
            for c in range(RW // LANES)
        ],
        axis=1,
    )
    retains = [jnp.exp(jnp.full((HD, HD), -decay[h], F32)) for h in range(HEADS)]
    for pair in range(GROUP // 2):
        shape = (2 * GROUP, 2 * LANES)
        pick = (
            lax.broadcasted_iota(jnp.int32, shape, 0) % GROUP
            == lane_iota(shape) // LANES + 2 * pair
        ).astype(BF16)
        columns = jnp.dot(kt, pick, preferred_element_type=F32)
        for i in range(2):
            b = 2 * pair + i
            for h in range(HEADS):
                column = columns[h * HD : (h + 1) * HD, i * LANES : i * LANES + HD]
                c = (h // 2) * LANES
                row = (swapped if h % 2 else v)[b : b + 1, c : c + HD]
                new_ref[b, h] = retains[h] * state_ref[b, h] + column * row


def expert_kernel(in_ref, wg_ref, wu_ref, wd_ref, out_hbm, wide, lhs, out, sem):
    n = 2 * EXPERTS
    for i in range(n):
        wide[i * STEP : i * STEP + TILES, :] = in_ref[i].astype(F32)
    for r in range(TILES):
        lhs[:, r * LANES : (r + 1) * LANES] = wide[pl.ds(r, n, stride=STEP), :].astype(BF16)
    rows = lhs[...]
    gate = jnp.dot(rows, wg_ref[0], preferred_element_type=F32)
    up = jnp.dot(rows, wu_ref[0], preferred_element_type=F32)
    hidden = (jax.nn.silu(gate) * up).astype(BF16)
    result = jnp.dot(hidden, wd_ref[0], preferred_element_type=F32)
    for r in range(TILES):
        wide[pl.ds(r, n, stride=STEP), :] = result[:, r * LANES : (r + 1) * LANES]
    copies = []
    for c in range(COPIES):
        for i in range(c * n // COPIES, (c + 1) * n // COPIES):
            k = 2 * OUT_ORDER.index(BACK_ORDER[i // 2]) + i % 2
            out[i] = wide[k * STEP : k * STEP + TILES, :].astype(BF16)
        rows = pl.ds(c * n // COPIES, n // COPIES)
        copy = pltpu.make_async_copy(out.at[rows], out_hbm.at[rows], sem.at[c])
        copy.start()
        copies.append(copy)
    for copy in copies:
        copy.wait()


def combine_kernel(slot, weight, mixed_ref, back_ref, out_hbm, wide, out, sem):
    copies = []
    for i in range(ROWS // PART):
        for t in range(i * PART, (i + 1) * PART):
            total = mixed_ref[t].astype(F32)
            for j in range(2):
                total = total + back_ref[slot[j, t]].astype(F32) * weight[j, t]
            wide[t * STEP : t * STEP + TILES, :] = total
        rows = pl.ds(i * PART, PART)
        for r in range(TILES):
            out[rows, r * LANES : (r + 1) * LANES] = wide[
                pl.ds(i * PART * STEP + r, PART, stride=STEP), :
            ].astype(BF16)
        copy = pltpu.make_async_copy(out.at[rows], out_hbm.at[rows], sem.at[i])
        copy.start()
        copies.append(copy)
    for copy in copies:
        copy.wait()


def in_vmem(x):
    return pltpu.with_memory_space_constraint(x, pltpu.VMEM)


def in_smem(x):
    return pltpu.with_memory_space_constraint(x, pltpu.SMEM)


def in_hbm(x):
    return pltpu.with_memory_space_constraint(x, pltpu.HBM)


HBM = pl.BlockSpec(memory_space=pltpu.HBM)
VMEM = pl.BlockSpec(memory_space=pltpu.VMEM)
SMEM = pl.BlockSpec(memory_space=pltpu.SMEM)
ROW_TILES = (2 * EXPERTS, TILES, LANES)


def local(
    tokens,
    history_length,
    norm_gain,
    w_query,
    w_key,
    w_value,
    w_gate,
    decay_rate,
    state,
    head_gain,
    w_out,
    moe_gain,
    route_weights,
    expert_group,
    expert_inner,
    expert_gate,
    expert_up,
    expert_down,
):
    inner = expert_inner.T
    inverse = jnp.asarray(
        (10000.0 ** (-(np.arange(LANES) % 32) / 32.0)).astype(np.float32).reshape(1, LANES)
    )
    mixed, send, keys, values, slots, weights, down = pl.pallas_call(
        front_kernel,
        out_shape=[
            pltpu.VMEM((ROWS, TILES, LANES), BF16),
            pltpu.VMEM(ROW_TILES, BF16),
            pltpu.VMEM((ROWS, RW), F32),
            pltpu.VMEM((ROWS, RW), F32),
            pltpu.SMEM((2, ROWS), jnp.int32),
            pltpu.SMEM((2, ROWS), F32),
            pltpu.VMEM(expert_down.shape, BF16),
        ],
        in_specs=[HBM] * 17,
        out_specs=[VMEM, VMEM, VMEM, VMEM, SMEM, SMEM, VMEM],
        scratch_shapes=[
            pltpu.VMEM((1, ROWS), jnp.int32),
            pltpu.VMEM((1, LANES), F32),
            pltpu.VMEM((1, D), F32),
            pltpu.SMEM((HEADS,), F32),
            pltpu.VMEM((1, RW), F32),
            pltpu.VMEM((TILES, LANES), F32),
            pltpu.SMEM((ROWS,), jnp.int32),
            pltpu.SMEM((2, ROWS), jnp.int32),
            pltpu.SMEM((EXPERTS,), jnp.int32),
            pltpu.SMEM((2, ROWS), jnp.int32),
            pltpu.VMEM((ROWS, D), BF16),
            pltpu.VMEM((4, D, RW), BF16),
            pltpu.VMEM((RW, D), BF16),
            pltpu.VMEM((ROWS, HEADS, HD, HD), F32),
            pltpu.VMEM((2, ROWS, RW), F32),
            pltpu.VMEM(((HEADS + 1) * ROWS, LANES), F32),
            pltpu.VMEM((ROWS * STEP, LANES), F32),
            pltpu.VMEM((ROWS, LANES), F32),
            pltpu.SemaphoreType.DMA((10,)),
            pltpu.SemaphoreType.DMA((6,)),
            pltpu.SemaphoreType.DMA((CHUNKS,)),
        ],
        compiler_params=pltpu.CompilerParams(vmem_limit_bytes=32 * 2**20),
        name="front",
    )(
        *(
            in_hbm(x)
            for x in (
                history_length.reshape(1, ROWS),
                inverse,
                norm_gain.reshape(1, D),
                decay_rate,
                head_gain.reshape(1, RW),
                moe_gain.reshape(TILES, LANES),
                expert_group,
                inner,
                route_weights.T,
                tokens,
                w_query,
                w_key,
                w_value,
                w_gate,
                state,
                w_out,
                expert_down,
            )
        )
    )

    new_state = pl.pallas_call(
        state_kernel,
        grid=(CHUNKS,),
        out_shape=jax.ShapeDtypeStruct(state.shape, F32),
        in_specs=[
            SMEM,
            pl.BlockSpec((GROUP, HEADS, HD, HD), lambda i: (i, 0, 0, 0)),
            pl.BlockSpec((GROUP, RW), lambda i: (i, 0)),
            pl.BlockSpec((GROUP, RW), lambda i: (i, 0)),
        ],
        out_specs=pl.BlockSpec((GROUP, HEADS, HD, HD), lambda i: (i, 0, 0, 0)),
        cost_estimate=pl.CostEstimate(
            flops=10**9, bytes_accessed=26 * 10**6, transcendentals=0
        ),
        compiler_params=pltpu.CompilerParams(vmem_limit_bytes=20 * 2**20),
        name="state_update",
    )(in_hbm(decay_rate), in_hbm(state), in_vmem(keys), in_vmem(values))

    def exchange(rows, order):
        return lax.all_to_all(
            rows,
            "ep",
            split_axis=0,
            concat_axis=0,
            axis_index_groups=[order],
            tiled=True,
        )

    outputs = pl.pallas_call(
        expert_kernel,
        out_shape=jax.ShapeDtypeStruct(ROW_TILES, BF16),
        in_specs=[VMEM] * 4,
        out_specs=HBM,
        scratch_shapes=[
            pltpu.VMEM((2 * EXPERTS * STEP, LANES), F32),
            pltpu.VMEM((2 * EXPERTS, D), BF16),
            pltpu.VMEM(ROW_TILES, BF16),
            pltpu.SemaphoreType.DMA((COPIES,)),
        ],
        cost_estimate=pl.CostEstimate(
            flops=8 * 10**8, bytes_accessed=4 * 10**6, transcendentals=0
        ),
        compiler_params=pltpu.CompilerParams(vmem_limit_bytes=16 * 2**20),
        name="expert",
    )(
        in_vmem(exchange(send, OUT_ORDER)),
        in_vmem(expert_gate),
        in_vmem(expert_up),
        in_vmem(down),
    )
    output = pl.pallas_call(
        combine_kernel,
        out_shape=jax.ShapeDtypeStruct((ROWS, D), BF16),
        in_specs=[SMEM, SMEM, VMEM, VMEM],
        out_specs=HBM,
        scratch_shapes=[
            pltpu.VMEM((ROWS * STEP, LANES), F32),
            pltpu.VMEM((ROWS, D), BF16),
            pltpu.SemaphoreType.DMA((ROWS // PART,)),
        ],
        compiler_params=pltpu.CompilerParams(vmem_limit_bytes=8 * 2**20),
        name="combine",
    )(in_smem(slots), in_smem(weights), in_vmem(mixed), in_vmem(exchange(outputs, BACK_ORDER)))
    return output, new_state


def solution(mesh):
    return jax.shard_map(
        local,
        mesh=mesh,
        in_specs=(
            P("ep", None),
            P("ep"),
            P(),
            P(),
            P(),
            P(),
            P(),
            P(),
            P("ep", None, None, None),
            P(),
            P(),
            P(),
            P("ep", None),
            P("ep"),
            P("ep", None),
            P("ep", None, None),
            P("ep", None, None),
            P("ep", None, None),
        ),
        out_specs=(P("ep", None), P("ep", None, None, None)),
        check_vma=False,
    )
```

```python
import functools

import jax
import jax.numpy as jnp
import numpy as np
from jax import lax
from jax.experimental import pallas as pl
from jax.experimental.pallas import tpu as pltpu
from jax.sharding import PartitionSpec as P

EPS = 1e-06
ROWS = 48
D = 2048
HEADS = 8
HD = 64
RW = HEADS * HD
EXPERTS = 128
LANES = 128
TILES = D // LANES
GROUP = 8
CHUNKS = ROWS // GROUP
PIECE = 4
PIECES = ROWS // PIECE
STEP = 20
PART = 16
COPIES = 4
F32 = jnp.float32
BF16 = jnp.bfloat16


SHIFT = 21
OUT_ORDER = [
    ((p % 4) * 32 + (p // 4 % 4) * 8 + (p // 16 % 4) * 2 + p // 64) ^ SHIFT
    for p in range(128)
]
BACK_ORDER = [
    (p % 4) * 32 + (p // 16 % 4) * 8 + (p // 4 % 4) * 2 + p // 64 for p in range(128)
]


def out_place(group, inner):
    inner = inner ^ SHIFT
    return group + (inner >> 3) * 4 + (inner >> 1 & 3) * 16 + (inner & 1) * 64


def back_place(group, inner):
    return group + (inner >> 1 & 3) * 4 + (inner >> 3) * 16 + (inner & 1) * 64


def lane_iota(shape):
    return lax.broadcasted_iota(jnp.int32, shape, len(shape) - 1)


def row_iota(shape):
    return lax.broadcasted_iota(jnp.int32, shape, 0)


def split(x):
    high = x.astype(BF16).astype(F32)
    return high, x - high


def by_lanes(f, x):
    return jnp.concatenate(
        [f(x[:, c * LANES : (c + 1) * LANES]) for c in range(x.shape[1] // LANES)],
        axis=1,
    )


def head_sum(x):
    shape = (LANES, LANES)
    ones = (row_iota(shape) // HD == lane_iota(shape) // HD).astype(BF16)

    def part(y):
        high, low = split(y)
        return jnp.dot(high.astype(BF16), ones, preferred_element_type=F32) + jnp.dot(
            low.astype(BF16), ones, preferred_element_type=F32
        )

    return by_lanes(part, x)


def rope(x, cosine, sine):
    first = (lane_iota((ROWS, LANES)) % HD) < (HD // 2)

    def part(y):
        other = jnp.where(
            first, pltpu.roll(y, LANES - HD // 2, 1), pltpu.roll(y, HD // 2, 1)
        )
        return y * cosine + other * sine

    return by_lanes(part, x)


def front_kernel(
    hist_hbm,
    inv_hbm,
    ngain_hbm,
    decay_hbm,
    hgain_hbm,
    mgain_hbm,
    group_hbm,
    inner_hbm,
    weight_hbm,
    tok_hbm,
    wq_hbm,
    wk_hbm,
    wv_hbm,
    wg_hbm,
    state_hbm,
    wo_hbm,
    down_hbm,
    mixed_ref,
    send_ref,
    k_ref,
    v_ref,
    slot_ref,
    weight_ref,
    down_ref,
    hist,
    inv,
    ngain,
    decay,
    hgain,
    mgain,
    group,
    inner,
    seen,
    target,
    tok,
    w4,
    wo,
    st,
    qs,
    part,
    wide,
    scales,
    small_sem,
    w_sem,
    st_sem,
):
    small = [
        pltpu.make_async_copy(src, dst, small_sem.at[i])
        for i, (src, dst) in enumerate(
            (
                (tok_hbm, tok),
                (ngain_hbm, ngain),
                (hist_hbm, hist),
                (inv_hbm, inv),
                (decay_hbm, decay),
                (hgain_hbm, hgain),
                (mgain_hbm, mgain),
                (group_hbm, group),
                (inner_hbm, inner),
                (weight_hbm, weight_ref),
            )
        )
    ]
    weights = [
        pltpu.make_async_copy(src, w4.at[i], w_sem.at[i])
        for i, src in enumerate((wq_hbm, wk_hbm, wv_hbm, wg_hbm))
    ]
    wo_copy = pltpu.make_async_copy(wo_hbm, wo, w_sem.at[4])
    down_copy = pltpu.make_async_copy(down_hbm, down_ref, w_sem.at[5])

    def state_copy(i):
        rows = pl.ds(i * PIECE, PIECE)
        return pltpu.make_async_copy(state_hbm.at[rows], st.at[rows], st_sem.at[i])

    for copy in small:
        copy.start()
    for copy in weights:
        copy.start()
    for copy in small:
        copy.wait()
    for i in range(2):
        state_copy(i).start()

    x = tok[...].astype(F32)
    scale = lax.rsqrt(jnp.mean(x * x, axis=-1, keepdims=True) + EPS)
    normed = (x * scale * ngain[...]).astype(BF16)

    square = (ROWS, ROWS)
    place = jnp.sum(
        jnp.where(
            row_iota(square) == lane_iota(square),
            jnp.broadcast_to(hist[...].astype(F32), square),
            0.0,
        ),
        axis=1,
        keepdims=True,
    )
    angles = place * inv[...]
    cosine = jnp.cos(angles)
    sine = jnp.sin(angles)
    sine = jnp.where((lane_iota((ROWS, LANES)) % HD) < (HD // 2), -sine, sine)

    for e in range(EXPERTS):
        seen[e] = 0
    for t in range(ROWS):
        for j in range(2):
            e = out_place(group[t], inner[j, t])
            slot = seen[e]
            seen[e] = 1
            target[j, t] = 2 * e + slot
            slot_ref[j, t] = 2 * back_place(group[t], inner[j, t]) + slot
    zero = jnp.zeros((TILES, LANES), BF16)
    for e in range(2 * EXPERTS):
        send_ref[e] = zero

    def project(i):
        weights[i].wait()
        return jnp.dot(normed, w4[i], preferred_element_type=F32).astype(BF16).astype(F32)

    q = project(0)
    for i in range(2, 6):
        state_copy(i).start()
    q = rope(q, cosine, sine)
    k = project(1)
    for i in range(6, PIECES):
        state_copy(i).start()
    wo_copy.start()
    k = rope(k, cosine, sine) * (HD**-0.5)
    v = project(2)
    down_copy.start()
    gate = project(3)
    for i, piece in enumerate(split(q)):
        qs[i] = piece
    k_ref[...] = k
    v_ref[...] = v

    fresh = head_sum(q * k) * v
    heads = lane_iota((1, RW)) // HD
    rate = jnp.zeros((1, RW), F32)
    for h in range(HEADS):
        rate = jnp.where(heads == h, decay[h], rate)
    retain = jnp.exp(-rate)
    own = row_iota((HEADS, RW)) == lane_iota((HEADS, RW)) // HD

    def read(t):
        spread = [
            jnp.where(own, jnp.broadcast_to(qs[s, pl.ds(t, 1), :], (HEADS, RW)), 0.0)
            for s in range(2)
        ]
        total = jnp.dot(
            jnp.concatenate(spread, axis=0).astype(BF16),
            st[t].reshape(RW, HD).astype(BF16),
            preferred_element_type=F32,
        )
        part[pl.ds(t * (HEADS + 1), HEADS), 0:HD] = (
            total[0:HEADS] + total[HEADS:]
        )

    def chunk(i, carry):
        state_copy(i).wait()
        for b in range(PIECE):
            read(i * PIECE + b)
        return carry

    lax.fori_loop(0, PIECES, chunk, 0)

    def head_rows(h):
        return part[pl.ds(h, ROWS, stride=HEADS + 1), :]

    low_half = lane_iota((ROWS, LANES)) < HD
    old = jnp.concatenate(
        [
            jnp.where(
                low_half, head_rows(2 * c), pltpu.roll(head_rows(2 * c + 1), HD, 1)
            )
            for c in range(HEADS // 2)
        ],
        axis=1,
    )
    reading = retain * old + fresh
    mean_square = head_sum(reading * reading) * (1.0 / HD)
    reading = reading * lax.rsqrt(mean_square + EPS) * hgain[...]
    mixed_heads = (reading * jax.nn.silu(gate)).astype(BF16)
    wo_copy.wait()
    squares = jnp.zeros((ROWS, LANES), F32)
    for n in range(0, D, 2 * LANES):
        block = slice(n, n + 2 * LANES)
        mixed = tok[:, block].astype(F32) + jnp.dot(
            mixed_heads, wo[:, block], preferred_element_type=F32
        )
        mixed = mixed.astype(BF16).astype(F32)
        for i in range(2):
            piece = mixed[:, i * LANES : (i + 1) * LANES]
            squares = squares + piece * piece
            wide[pl.ds(n // LANES + i, ROWS, stride=STEP), :] = piece
    scale = lax.rsqrt(jnp.sum(squares, axis=-1, keepdims=True) * (1.0 / D) + EPS)
    scales[...] = jnp.broadcast_to(scale, (ROWS, LANES))
    for t in range(ROWS):
        tile = wide[t * STEP : t * STEP + TILES, :]
        mixed_ref[t] = tile.astype(BF16)
        row = (tile * scales[t : t + 1, :] * mgain[...]).astype(BF16)
        for j in range(2):
            send_ref[target[j, t]] = row
    down_copy.wait()


def state_kernel(decay, state_ref, k_ref, v_ref, new_ref):
    k = k_ref[...]
    high = k.astype(BF16).astype(F32)
    kt = jnp.concatenate([high, k - high], axis=0).T.astype(BF16)
    v = v_ref[...]
    swapped = jnp.concatenate(
        [
            pltpu.roll(v[:, c * LANES : (c + 1) * LANES], HD, 1)
            for c in range(RW // LANES)
        ],
        axis=1,
    )
    retains = [jnp.exp(jnp.full((HD, HD), -decay[h], F32)) for h in range(HEADS)]
    for pair in range(GROUP // 2):
        shape = (2 * GROUP, 2 * LANES)
        pick = (
            lax.broadcasted_iota(jnp.int32, shape, 0) % GROUP
            == lane_iota(shape) // LANES + 2 * pair
        ).astype(BF16)
        columns = jnp.dot(kt, pick, preferred_element_type=F32)
        for i in range(2):
            b = 2 * pair + i
            for h in range(HEADS):
                column = columns[h * HD : (h + 1) * HD, i * LANES : i * LANES + HD]
                c = (h // 2) * LANES
                row = (swapped if h % 2 else v)[b : b + 1, c : c + HD]
                new_ref[b, h] = retains[h] * state_ref[b, h] + column * row


def expert_kernel(in_ref, wg_ref, wu_ref, wd_ref, out_hbm, wide, lhs, out, sem):
    n = 2 * EXPERTS
    for i in range(n):
        wide[i * STEP : i * STEP + TILES, :] = in_ref[i].astype(F32)
    for r in range(TILES):
        lhs[:, r * LANES : (r + 1) * LANES] = wide[pl.ds(r, n, stride=STEP), :].astype(BF16)
    rows = lhs[...]
    gate = jnp.dot(rows, wg_ref[0], preferred_element_type=F32)
    up = jnp.dot(rows, wu_ref[0], preferred_element_type=F32)
    hidden = (jax.nn.silu(gate) * up).astype(BF16)
    result = jnp.dot(hidden, wd_ref[0], preferred_element_type=F32)
    for r in range(TILES):
        wide[pl.ds(r, n, stride=STEP), :] = result[:, r * LANES : (r + 1) * LANES]
    copies = []
    for c in range(COPIES):
        for i in range(c * n // COPIES, (c + 1) * n // COPIES):
            k = 2 * OUT_ORDER.index(BACK_ORDER[i // 2]) + i % 2
            out[i] = wide[k * STEP : k * STEP + TILES, :].astype(BF16)
        rows = pl.ds(c * n // COPIES, n // COPIES)
        copy = pltpu.make_async_copy(out.at[rows], out_hbm.at[rows], sem.at[c])
        copy.start()
        copies.append(copy)
    for copy in copies:
        copy.wait()


def combine_kernel(slot, weight, mixed_ref, back_ref, out_hbm, wide, out, sem):
    copies = []
    for i in range(ROWS // PART):
        for t in range(i * PART, (i + 1) * PART):
            total = mixed_ref[t].astype(F32)
            for j in range(2):
                total = total + back_ref[slot[j, t]].astype(F32) * weight[j, t]
            wide[t * STEP : t * STEP + TILES, :] = total
        rows = pl.ds(i * PART, PART)
        for r in range(TILES):
            out[rows, r * LANES : (r + 1) * LANES] = wide[
                pl.ds(i * PART * STEP + r, PART, stride=STEP), :
            ].astype(BF16)
        copy = pltpu.make_async_copy(out.at[rows], out_hbm.at[rows], sem.at[i])
        copy.start()
        copies.append(copy)
    for copy in copies:
        copy.wait()


def in_vmem(x):
    return pltpu.with_memory_space_constraint(x, pltpu.VMEM)


def in_smem(x):
    return pltpu.with_memory_space_constraint(x, pltpu.SMEM)


def in_hbm(x):
    return pltpu.with_memory_space_constraint(x, pltpu.HBM)


HBM = pl.BlockSpec(memory_space=pltpu.HBM)
VMEM = pl.BlockSpec(memory_space=pltpu.VMEM)
SMEM = pl.BlockSpec(memory_space=pltpu.SMEM)
ROW_TILES = (2 * EXPERTS, TILES, LANES)


def local(
    tokens,
    history_length,
    norm_gain,
    w_query,
    w_key,
    w_value,
    w_gate,
    decay_rate,
    state,
    head_gain,
    w_out,
    moe_gain,
    route_weights,
    expert_group,
    expert_inner,
    expert_gate,
    expert_up,
    expert_down,
):
    inner = expert_inner.T
    inverse = jnp.asarray(
        (10000.0 ** (-(np.arange(LANES) % 32) / 32.0)).astype(np.float32).reshape(1, LANES)
    )
    mixed, send, keys, values, slots, weights, down = pl.pallas_call(
        front_kernel,
        out_shape=[
            pltpu.VMEM((ROWS, TILES, LANES), BF16),
            pltpu.VMEM(ROW_TILES, BF16),
            pltpu.VMEM((ROWS, RW), F32),
            pltpu.VMEM((ROWS, RW), F32),
            pltpu.SMEM((2, ROWS), jnp.int32),
            pltpu.SMEM((2, ROWS), F32),
            pltpu.VMEM(expert_down.shape, BF16),
        ],
        in_specs=[HBM] * 17,
        out_specs=[VMEM, VMEM, VMEM, VMEM, SMEM, SMEM, VMEM],
        scratch_shapes=[
            pltpu.VMEM((1, ROWS), jnp.int32),
            pltpu.VMEM((1, LANES), F32),
            pltpu.VMEM((1, D), F32),
            pltpu.SMEM((HEADS,), F32),
            pltpu.VMEM((1, RW), F32),
            pltpu.VMEM((TILES, LANES), F32),
            pltpu.SMEM((ROWS,), jnp.int32),
            pltpu.SMEM((2, ROWS), jnp.int32),
            pltpu.SMEM((EXPERTS,), jnp.int32),
            pltpu.SMEM((2, ROWS), jnp.int32),
            pltpu.VMEM((ROWS, D), BF16),
            pltpu.VMEM((4, D, RW), BF16),
            pltpu.VMEM((RW, D), BF16),
            pltpu.VMEM((ROWS, HEADS, HD, HD), F32),
            pltpu.VMEM((2, ROWS, RW), F32),
            pltpu.VMEM(((HEADS + 1) * ROWS, LANES), F32),
            pltpu.VMEM((ROWS * STEP, LANES), F32),
            pltpu.VMEM((ROWS, LANES), F32),
            pltpu.SemaphoreType.DMA((10,)),
            pltpu.SemaphoreType.DMA((6,)),
            pltpu.SemaphoreType.DMA((PIECES,)),
        ],
        compiler_params=pltpu.CompilerParams(vmem_limit_bytes=32 * 2**20),
        name="front",
    )(
        *(
            in_hbm(x)
            for x in (
                history_length.reshape(1, ROWS),
                inverse,
                norm_gain.reshape(1, D),
                decay_rate,
                head_gain.reshape(1, RW),
                moe_gain.reshape(TILES, LANES),
                expert_group,
                inner,
                route_weights.T,
                tokens,
                w_query,
                w_key,
                w_value,
                w_gate,
                state,
                w_out,
                expert_down,
            )
        )
    )

    new_state = pl.pallas_call(
        state_kernel,
        grid=(CHUNKS,),
        out_shape=jax.ShapeDtypeStruct(state.shape, F32),
        in_specs=[
            SMEM,
            pl.BlockSpec((GROUP, HEADS, HD, HD), lambda i: (i, 0, 0, 0)),
            pl.BlockSpec((GROUP, RW), lambda i: (i, 0)),
            pl.BlockSpec((GROUP, RW), lambda i: (i, 0)),
        ],
        out_specs=pl.BlockSpec((GROUP, HEADS, HD, HD), lambda i: (i, 0, 0, 0)),
        cost_estimate=pl.CostEstimate(
            flops=10**9, bytes_accessed=26 * 10**6, transcendentals=0
        ),
        compiler_params=pltpu.CompilerParams(vmem_limit_bytes=20 * 2**20),
        name="state_update",
    )(in_hbm(decay_rate), in_hbm(state), in_vmem(keys), in_vmem(values))

    def exchange(rows, order):
        return lax.all_to_all(
            rows,
            "ep",
            split_axis=0,
            concat_axis=0,
            axis_index_groups=[order],
            tiled=True,
        )

    outputs = pl.pallas_call(
        expert_kernel,
        out_shape=jax.ShapeDtypeStruct(ROW_TILES, BF16),
        in_specs=[VMEM] * 4,
        out_specs=HBM,
        scratch_shapes=[
            pltpu.VMEM((2 * EXPERTS * STEP, LANES), F32),
            pltpu.VMEM((2 * EXPERTS, D), BF16),
            pltpu.VMEM(ROW_TILES, BF16),
            pltpu.SemaphoreType.DMA((COPIES,)),
        ],
        cost_estimate=pl.CostEstimate(
            flops=8 * 10**8, bytes_accessed=4 * 10**6, transcendentals=0
        ),
        compiler_params=pltpu.CompilerParams(vmem_limit_bytes=16 * 2**20),
        name="expert",
    )(
        in_vmem(exchange(send, OUT_ORDER)),
        in_vmem(expert_gate),
        in_vmem(expert_up),
        in_vmem(down),
    )
    output = pl.pallas_call(
        combine_kernel,
        out_shape=jax.ShapeDtypeStruct((ROWS, D), BF16),
        in_specs=[SMEM, SMEM, VMEM, VMEM],
        out_specs=HBM,
        scratch_shapes=[
            pltpu.VMEM((ROWS * STEP, LANES), F32),
            pltpu.VMEM((ROWS, D), BF16),
            pltpu.SemaphoreType.DMA((ROWS // PART,)),
        ],
        compiler_params=pltpu.CompilerParams(vmem_limit_bytes=8 * 2**20),
        name="combine",
    )(in_smem(slots), in_smem(weights), in_vmem(mixed), in_vmem(exchange(outputs, BACK_ORDER)))
    return output, new_state


def solution(mesh):
    return jax.shard_map(
        local,
        mesh=mesh,
        in_specs=(
            P("ep", None),
            P("ep"),
            P(),
            P(),
            P(),
            P(),
            P(),
            P(),
            P("ep", None, None, None),
            P(),
            P(),
            P(),
            P("ep", None),
            P("ep"),
            P("ep", None),
            P("ep", None, None),
            P("ep", None, None),
            P("ep", None, None),
        ),
        out_specs=(P("ep", None), P("ep", None, None, None)),
        check_vma=False,
    )
```
